32 devices in a mesh: sp: 8 (over z, y), tp: 4 (over x, core).
Axes of the slice: x: 2, y: 2, z: 4, core: 2. Of those that a mesh axis runs over, the one named last changes fastest.
Arguments:
- stream_in: bfloat16 [4096, 2048], P(('sp', 'tp')), may hold values from -6 to 6
- stream_cot: bfloat16 [4096, 2048], P(('sp', 'tp')), may hold values from -4 to 4
- route_ids: int32 [4096, 2], P('sp'), may hold values from 0 to 7, all different within a row; in each aligned block of 128 rows (0 to 127, 128 to 255, ...) at most 40 rows name the same one
- route_wts: float32 [4096, 2], P('sp'), may hold values from 0.2 to 0.8
- norm_gain: float32 [2048], replicated, may hold values from 0.1 to 1.9
- w_gate: bfloat16 [8, 2048, 1024], P('sp', None, 'tp'), may hold values from -0.125 to 0.125
- w_up: bfloat16 [8, 2048, 1024], P('sp', None, 'tp'), may hold values from -0.125 to 0.125
- w_down: bfloat16 [8, 1024, 2048], P('sp', 'tp'), may hold values from -0.1875 to 0.1875
- out_proj: bfloat16 [1024, 2048], P('tp'), may hold values from -0.1875 to 0.1875
- conv_b: bfloat16 [4096, 1024], P('sp', 'tp'), may hold values from -6 to 6
- conv_c: bfloat16 [4096, 1024], P('sp', 'tp'), may hold values from -6 to 6
- conv_h: bfloat16 [4096, 1024], P('sp', 'tp'), may hold values from -6 to 6
- conv_taps: float32 [3, 1024], P(None, 'tp'), may hold values from -3.5 to 3.5
Outputs:
- grad_gate: float32 [8, 2048, 1024], P('sp', None, 'tp')
- grad_up: float32 [8, 2048, 1024], P('sp', None, 'tp')
- grad_down: float32 [8, 1024, 2048], P('sp', 'tp')
- proj_grad: float32 [2048, 1024], P('sp', 'tp')
- grad_b: bfloat16 [4096, 1024], P('sp', 'tp')
- grad_c: bfloat16 [4096, 1024], P('sp', 'tp')
- grad_h: bfloat16 [4096, 1024], P('sp', 'tp')
The draws below stay inside these ranges and needn't reach their ends.
Inputs may be any that keep to these rules, and one draw needn't show every extreme that they name: `route_ids`: the 2 experts of a token differ. In each aligned block of 128 tokens no expert is named by more than 40 pairs, and in every draw some expert is named by exactly 40 pairs of some block.
All inputs are finite; a program needn't handle non-finite values.
Results may differ from the reference program's by a relative error of at most 0.015.
Values may be sent and summed in bfloat16 or wider, within the bound.
A program may use at most 128 MiB of HBM per device.

```python
import math
import jax
import jax.numpy as jnp
import numpy as np
from jax import lax

D = 2048
SC_W = 1024
FF = 1024
TOPK = 2
TAPS = 3
TOK_DEV = 128
TOKENS = 4096
EXPERTS = 8
CAP = 40
N_SP = 8
N_TP = 4


def raised(drawn, rng, source, target, shards_of, factor):
    owner, partner = [(jnp.arange(drawn.shape[axis_at]) // (drawn.shape[axis_at] // shards_of)).reshape([-1 if axis == axis_at else 1 for axis in range(drawn.ndim)]) for axis_at in (source, target)]
    chosen = jax.random.permutation(rng, shards_of)[partner]
    strong = (owner == chosen) | (owner == (partner + shards_of // 2) % shards_of)
    return jnp.where(strong, factor * drawn, drawn)


def block_levels(rng, shape, split, least, largest):
    gain, own = 1.0, jax.random.fold_in(rng, 6)
    for dim, parts in split:
        draws = jnp.exp(jax.random.uniform(jax.random.fold_in(own, dim), (parts,), jnp.float32, least / len(split), largest / len(split)))
        gain = gain * jnp.repeat(draws, shape[dim] // parts).reshape([-1 if axis == dim else 1 for axis in range(len(shape))])
    return gain


def deal_out(own_key, own, number, rows, count, top, limit, lean):
    ranking = jax.random.permutation(own_key, count)
    crowded, ordinary = portions_of(count, rows * top, limit, lean, True), portions_of(count, rows * top, limit, lean, False)
    places = jnp.arange(count)

    def named(sizes, rotation):
        used = int((sizes > 0).sum())
        fixed = max(1, used // 4)
        passed = fixed + (places - fixed + rotation * (used - fixed)) % max(1, count - fixed)
        return jnp.zeros((count,), jnp.int32).at[ranking[jnp.where(places < fixed, places, passed)]].set(jnp.asarray(sizes, jnp.int32))

    sizes = jnp.where(number % 4 == 0, named(crowded, number // 4), named(ordinary, number - number // 4 - 1))
    mixed = jax.random.permutation(jax.random.fold_in(own, 3), count)
    source_of, taker = mixed[0:count // 2 * 2:2], mixed[1:count // 2 * 2:2]
    slack = jnp.minimum(sizes[source_of] - 1, limit - sizes[taker]) // 2
    slack = jnp.where((source_of == ranking[0]) | (taker == ranking[0]) | (sizes[taker] == 0), 0, jnp.maximum(slack, 0))
    passed = jax.random.randint(jax.random.fold_in(own, 4), (count // 2,), 0, 1 << 20) % (slack + 1)
    sizes = sizes.at[source_of].add(-passed).at[taker].add(passed)
    members = jnp.searchsorted(jnp.cumsum(sizes), jnp.arange(rows * top), side="right").astype(jnp.int32)
    table = members.reshape(top, rows).T
    table = table[jax.random.permutation(jax.random.fold_in(own, 1), rows)]
    rotation = jax.random.randint(jax.random.fold_in(own, 2), (rows, 1), 0, top)
    return jnp.take_along_axis(table, (jnp.arange(top)[None, :] + rotation) % top, axis=1)


def portions_of(count, total, most, lean, full):
    portions = [(1 << 20) // math.isqrt(rank ** lean) + 1 for rank in range(1, count + 1)]
    largest = most if full else min(most, max(-(-total // count), total * portions[0] // sum(portions)))
    least = 1 if total - largest >= count - 1 else 0
    counts, rest = [largest] + [least] * (count - 1), total - largest - least * (count - 1)
    while rest > 0:
        candidates = [i for i in range(1, count) if counts[i] < largest] or [i for i in range(1, count) if counts[i] < most]
        mass, budget = sum([portions[i] for i in candidates]), rest
        for i in candidates:
            extra = min(most - counts[i], max(1, budget * portions[i] // mass), rest)
            counts[i] = counts[i] + extra
            rest = rest - extra
    return np.array(counts)


def scatter_about(rng, shape, spread, most, cuts=(), held_as=jnp.bfloat16):
    gain = block_levels(rng, shape, cuts, -0.22, 0.18) if cuts else 1.0
    array = jax.random.normal(rng, shape, jnp.float32) * spread * gain
    return jnp.minimum(jnp.maximum(array, -most), most).astype(held_as)


def noise_with(own_key, dims, scale, most, cuts, heavy, held_as=jnp.bfloat16):
    values = scale * jax.random.normal(own_key, dims, jnp.float32)
    if cuts:
        values = values * block_levels(own_key, dims, cuts, -0.22, 0.18)
    return jnp.clip(raised(values, jax.random.fold_in(own_key, 3), *heavy), -most, most).astype(held_as)


def setup_inputs(seed: int = 0) -> dict:
    key_list = jax.random.split(jax.random.key(seed), 14)
    stream_in = scatter_about(key_list[0], (TOKENS, D), 1.0, 6.0, ((0, 32),))
    stream_cot = noise_with(key_list[1], (TOKENS, D), 0.5, 4.0, ((0, 32),), (0, 1, 32, 2.75))
    route_ids_keys = jax.random.split(jax.random.fold_in(key_list[2], 1), TOKENS // TOK_DEV)
    route_ids_turns = jax.random.permutation(jax.random.fold_in(key_list[2], 3), TOKENS // TOK_DEV)
    route_ids = jax.vmap(lambda own, number: deal_out(jax.random.fold_in(key_list[2], 2), own, number, TOK_DEV, EXPERTS, TOPK, CAP, 1))(route_ids_keys, route_ids_turns).reshape((TOKENS, TOPK))
    route_wts = jnp.clip(0.2 + 0.6 * jax.random.uniform(key_list[3], (TOKENS, TOPK), jnp.float32) ** block_levels(key_list[3], (TOKENS, TOPK), ((0, 8),), -0.2, 0.2), 0.2, 0.8)
    norm_gain = jnp.clip(1.0 + 0.18 * jax.random.normal(key_list[4], (D,), jnp.float32), 0.1, 1.9)
    w_gate = scatter_about(key_list[5], (EXPERTS, D, FF), D ** -0.5, 0.125, ((0, 8), (2, 4)))
    w_up = scatter_about(key_list[6], (EXPERTS, D, FF), D ** -0.5, 0.125, ((0, 8), (2, 4)))
    w_down = scatter_about(key_list[7], (EXPERTS, FF, D), FF ** -0.5, 0.1875, ((0, 8), (1, 4)))
    out_proj = scatter_about(key_list[8], (SC_W, D), SC_W ** -0.5, 0.1875, ((0, 4),))
    conv_b = scatter_about(key_list[9], (TOKENS, SC_W), 1.0, 6.0, ((0, 8), (1, 4)))
    conv_c = scatter_about(key_list[10], (TOKENS, SC_W), 1.0, 6.0, ((0, 8), (1, 4)))
    conv_h = scatter_about(key_list[11], (TOKENS, SC_W), 1.0, 6.0, ((0, 8), (1, 4)))
    conv_taps = scatter_about(key_list[12], (TAPS, SC_W), TAPS ** -0.5, 3.5, ((1, 4),), jnp.float32)
    return dict(stream_in=stream_in, stream_cot=stream_cot, route_ids=route_ids, route_wts=route_wts, norm_gain=norm_gain, w_gate=w_gate, w_up=w_up, w_down=w_down, out_proj=out_proj, conv_b=conv_b, conv_c=conv_c, conv_h=conv_h, conv_taps=conv_taps)


epsilon = 1e-06

def rounded(value):
    return lax.optimization_barrier(value.astype(jnp.bfloat16)).astype(jnp.float32)

def mmul(left, right):
    return jnp.dot(left, right, precision=lax.Precision.HIGHEST)

def reference(stream_in, stream_cot, route_ids, route_wts, norm_gain, w_gate, w_up, w_down, out_proj, conv_b, conv_c, conv_h, conv_taps):
    inputs = stream_in.astype(jnp.float32)
    inv_rms = lax.rsqrt(lax.optimization_barrier(jnp.mean(inputs * inputs, axis=1, keepdims=True)) + epsilon)
    scaled = inputs * inv_rms
    normed = (scaled * norm_gain[None, :]).astype(jnp.bfloat16)
    device_count = N_SP * N_TP
    pair_count = TOPK * TOKENS
    ids_device = route_ids.reshape(device_count, TOPK * TOK_DEV)
    onehot = (ids_device[:, :, None] == jnp.arange(EXPERTS, dtype=jnp.int32)).astype(jnp.int32)
    slot_rank = lax.optimization_barrier(jnp.sum((jnp.cumsum(onehot, axis=1) - 1) * onehot, axis=2))
    device_idx = jnp.arange(device_count, dtype=jnp.int32)[:, None]
    per_expert = device_count * CAP
    position = ids_device * per_expert + device_idx * CAP + slot_rank
    slot_table = jnp.full((EXPERTS * per_expert,), pair_count, jnp.int32)
    slot_table = slot_table.at[position.reshape(-1)].set(jnp.arange(pair_count, dtype=jnp.int32))
    slot_table = slot_table.reshape(EXPERTS, per_expert)
    zero_row = jnp.zeros((1, D), jnp.bfloat16)
    normed_pad = jnp.concatenate([normed, zero_row], axis=0)
    cot_pad = jnp.concatenate([stream_cot, zero_row], axis=0)
    wts_pad = jnp.concatenate([route_wts.reshape(-1), jnp.zeros((1,), jnp.float32)])
    ff_block = FF // N_TP

    def one_expert(grad_total, expert_in):
        pair_rows, gate_w, up_w, down_w = expert_in
        token_rows = pair_rows // TOPK
        rows_in = normed_pad[token_rows].astype(jnp.float32)
        cot_rows = rounded(wts_pad[pair_rows][:, None] * cot_pad[token_rows].astype(jnp.float32))
        gate_f = gate_w.astype(jnp.float32)
        up_f = up_w.astype(jnp.float32)
        down_f = down_w.astype(jnp.float32)
        gate_pre = mmul(rows_in, gate_f)
        up_pre = mmul(rows_in, up_f)
        gate_sig = jax.nn.sigmoid(gate_pre)
        gate_act = gate_pre * gate_sig
        hidden = rounded(gate_act * up_pre)
        down_grad = mmul(hidden.T, cot_rows)
        grad_hidden = mmul(cot_rows, down_f.T)
        up_grad = rounded(grad_hidden * gate_act)
        gate_grad = rounded(grad_hidden * up_pre * gate_sig * (1.0 + gate_pre * (1.0 - gate_sig)))
        gate_wgrad = mmul(rows_in.T, gate_grad)
        up_wgrad = mmul(rows_in.T, up_grad)
        back_sum = jnp.zeros((rows_in.shape[0], D), jnp.float32)
        for block_idx in range(N_TP):
            low = block_idx * ff_block
            high = low + ff_block
            partial_back = mmul(gate_grad[:, low:high], gate_f[:, low:high].T) + mmul(up_grad[:, low:high], up_f[:, low:high].T)
            back_sum = back_sum + rounded(partial_back)
        back_rows = rounded(back_sum)
        grad_total = grad_total.at[token_rows].add(back_rows)
        return (grad_total, (gate_wgrad, up_wgrad, down_grad))
    start_total = jnp.zeros((TOKENS + 1, D), jnp.float32)
    grad_total, expert_grads = lax.scan(one_expert, start_total, (slot_table, w_gate, w_up, w_down))
    grad_gate, grad_up, grad_down = expert_grads
    grad_normed = grad_total[:TOKENS]
    q_term = grad_normed * norm_gain[None, :]
    stream_grad = (stream_cot.astype(jnp.float32) + inv_rms * (q_term - scaled * lax.optimization_barrier(jnp.mean(q_term * scaled, axis=1, keepdims=True)))).astype(jnp.bfloat16)
    grad_mix = jnp.dot(stream_grad, out_proj.T, preferred_element_type=jnp.float32).astype(jnp.bfloat16)
    conv_in = conv_c.astype(jnp.float32) * conv_h.astype(jnp.float32)
    padded_in = jnp.pad(conv_in, ((2, 0), (0, 0)))
    conv_out = conv_taps[0][None, :] * padded_in[:-2] + conv_taps[1][None, :] * padded_in[1:-1] + conv_taps[2][None, :] * padded_in[2:]
    mixed = (conv_b.astype(jnp.float32) * conv_out).astype(jnp.bfloat16)
    proj_grad = jnp.dot(stream_grad.T, mixed, preferred_element_type=jnp.float32)
    grad_b = (grad_mix.astype(jnp.float32) * conv_out).astype(jnp.bfloat16)
    conv_grad = grad_mix.astype(jnp.float32) * conv_b.astype(jnp.float32)
    padded_grad = jnp.pad(conv_grad, ((0, 2), (0, 0)))
    grad_in = conv_taps[2][None, :] * padded_grad[:-2] + conv_taps[1][None, :] * padded_grad[1:-1] + conv_taps[0][None, :] * padded_grad[2:]
    grad_c = (grad_in * conv_h.astype(jnp.float32)).astype(jnp.bfloat16)
    grad_h = (grad_in * conv_c.astype(jnp.float32)).astype(jnp.bfloat16)
    return (grad_gate, grad_up, grad_down, proj_grad, grad_b, grad_c, grad_h)
```

```python
import functools

import jax
import jax.numpy as jnp
from jax import lax
from jax.experimental import pallas as pl
from jax.experimental.pallas import tpu as pltpu
from jax.sharding import PartitionSpec as P

epsilon = 1e-06


def here():
    return lax.axis_index("sp"), lax.axis_index("tp")


def greet(sp_count, tp_count):
    sp_at, tp_at = here()
    half = tp_count // 2
    barrier = pltpu.get_barrier_semaphore()

    def hail(sp_to, tp_to):
        pl.semaphore_signal(
            barrier, inc=1, device_id=(sp_to, tp_to), device_id_type=pl.DeviceIdType.MESH
        )

    def hail_row(step, carry):
        hail(lax.rem(sp_at + step, sp_count), tp_at)
        return carry

    lax.fori_loop(1, sp_count, hail_row, 0)
    for step in range(1, half):
        hail(sp_at, pair_peer(tp_at, step, half))
    hail(sp_at, mate_of(tp_at))
    pl.semaphore_wait(barrier, sp_count - 1 + half)


def pair_peer(tp_at, step, half):
    return lax.rem(tp_at // 2 + step, half) * 2 + lax.rem(tp_at, 2)


def mate_of(tp_at):
    return tp_at + 1 - 2 * lax.rem(tp_at, 2)


def remote(source, target, send_sem, recv_sem, sp_to, tp_to):
    return pltpu.make_async_remote_copy(
        src_ref=source,
        dst_ref=target,
        send_sem=send_sem,
        recv_sem=recv_sem,
        device_id=(sp_to, tp_to),
        device_id_type=pl.DeviceIdType.MESH,
    )


def loop(first, last, body):
    def step(index, carry):
        body(index)
        return carry

    lax.fori_loop(first, last, step, 0)


def spread_kernel(sp_count, tp_count, exchanged, gathered, *refs):
    count = exchanged + gathered
    sources, results = refs[:count], refs[count : 2 * count]
    own_sem, row_send, row_recv, pair_send, pair_recv, mate_send, mate_recv, last_send, last_recv = (
        refs[2 * count :]
    )
    sp_at, tp_at = here()
    half = tp_count // 2
    mate = mate_of(tp_at)

    def origin(step):
        return lax.rem(sp_at + sp_count - step, sp_count)

    def slot_of(which, step, tp_from):
        if which < exchanged:
            return results[which].at[origin(step), tp_from]
        return results[which].at[tp_from]

    def own_block(which):
        return sources[which].at[sp_at] if which < exchanged else sources[which]

    def row_copy(which, step):
        to = lax.rem(sp_at + step, sp_count)
        return remote(
            sources[which].at[to],
            results[which].at[sp_at, tp_at],
            row_send.at[which, step],
            row_recv.at[which, step],
            to,
            tp_at,
        )

    def row_arrival(which, step):
        return remote(
            own_block(which),
            slot_of(which, step, tp_at),
            row_send.at[which, step],
            row_recv.at[which, step],
            origin(step),
            tp_at,
        )

    def pair_copy(which, step, hop, source, tp_from):
        return remote(
            source,
            slot_of(which, step, tp_from),
            pair_send.at[which, step, hop],
            pair_recv.at[which, step, hop],
            sp_at,
            pair_peer(tp_at, hop, half),
        )

    def mate_copy(which, step, source, tp_from):
        return remote(
            source,
            slot_of(which, step, tp_from),
            mate_send.at[which, step],
            mate_recv.at[which, step],
            sp_at,
            mate,
        )

    def last_copy(which, step, hop, tp_from):
        return remote(
            slot_of(which, step, tp_from),
            slot_of(which, step, tp_from),
            last_send.at[which, step, hop],
            last_recv.at[which, step, hop],
            sp_at,
            mate,
        )

    def pair_source(hop):
        return pair_peer(tp_at, half - hop, half)

    def pass_on(which, step, source):
        for hop in range(1, half):
            pair_copy(which, step, hop, source, tp_at).start()
        mate_copy(which, step, source, tp_at).start()

    def pass_last(which, step):
        for hop in range(1, half):
            origin_tp = pair_source(hop)
            pair_copy(which, step, hop, own_block(which), origin_tp).wait_recv()
            last_copy(which, step, hop, origin_tp).start()

    greet(sp_count, tp_count)
    for which in range(exchanged):
        loop(1, sp_count, lambda step: row_copy(which, step).start())
    locals_ = [
        pltpu.make_async_copy(own_block(which), slot_of(which, 0, tp_at), own_sem.at[which])
        for which in range(count)
    ]
    for copy in locals_:
        copy.start()
    for which in reversed(range(count)):
        pass_on(which, 0, own_block(which))

    for which in range(exchanged, count):
        pass_last(which, 0)
    for which in range(exchanged):

        def relay(step):
            row_arrival(which, step).wait_recv()
            pass_on(which, step, slot_of(which, step, tp_at))
            pass_last(which, step - 1)

        loop(1, sp_count, relay)
        pass_last(which, sp_count - 1)

    for copy in locals_:
        copy.wait()
    for which in range(count):
        steps = sp_count if which < exchanged else 1

        def finish(step):
            for hop in range(1, half):
                pair_copy(which, step, hop, own_block(which), tp_at).wait_send()
                last_copy(which, step, hop, pair_source(hop)).wait_send()
                last_copy(
                    which, step, hop, mate_of(pair_source(hop))
                ).wait_recv()
            mate_copy(which, step, own_block(which), tp_at).wait_send()
            mate_copy(which, step, own_block(which), mate).wait_recv()

        loop(0, steps, finish)
        if which < exchanged:
            loop(1, sp_count, lambda step: row_copy(which, step).wait_send())


def spread(sp_count, tp_count, exchanged, gathered, collective_id):
    arrays = list(exchanged) + list(gathered)
    count = len(arrays)
    half = tp_count // 2
    shapes = [
        jax.ShapeDtypeStruct((sp_count, tp_count) + value.shape[1:], value.dtype)
        for value in exchanged
    ] + [jax.ShapeDtypeStruct((tp_count,) + value.shape, value.dtype) for value in gathered]
    sems = pltpu.SemaphoreType.DMA
    return pl.pallas_call(
        functools.partial(spread_kernel, sp_count, tp_count, len(exchanged), len(gathered)),
        out_shape=tuple(shapes),
        in_specs=[pl.BlockSpec(memory_space=pltpu.VMEM)] * count,
        out_specs=tuple([pl.BlockSpec(memory_space=pl.ANY)] * count),
        scratch_shapes=[sems((count,))]
        + [sems((count, sp_count))] * 2
        + [sems((count, sp_count, half))] * 2
        + [sems((count, sp_count))] * 2
        + [sems((count, sp_count, half))] * 2,
        compiler_params=pltpu.CompilerParams(collective_id=collective_id, has_side_effects=True),
    )(*arrays)


def bring_kernel(
    sp_count,
    tp_count,
    partial_ref,
    result_ref,
    own,
    from_mate,
    from_pair,
    final,
    load_sem,
    mate_send,
    mate_recv,
    pair_send,
    pair_recv,
    row_send,
    row_recv,
    own_sem,
):
    sp_at, tp_at = here()
    half = tp_count // 2
    pair_at, side = tp_at // 2, lax.rem(tp_at, 2)
    mate = mate_of(tp_at)

    def target(step):
        return lax.rem(sp_at + step, sp_count)

    def load(step):
        return pltpu.make_async_copy(
            partial_ref.at[target(step), :, side], own.at[step], load_sem.at[step]
        )

    def mate_copy(step):
        return remote(
            partial_ref.at[target(step), :, 1 - side],
            from_mate.at[step],
            mate_send.at[step],
            mate_recv.at[step],
            sp_at,
            mate,
        )

    def pair_copy(step, hop):
        return remote(
            own.at[step, lax.rem(pair_at + hop, half)],
            from_pair.at[step, hop - 1],
            pair_send.at[step, hop],
            pair_recv.at[step, hop],
            sp_at,
            pair_peer(tp_at, hop, half),
        )

    def row_copy(step):
        return remote(
            final.at[step],
            result_ref.at[sp_at],
            row_send.at[step],
            row_recv.at[step],
            target(step),
            tp_at,
        )

    def row_arrival(step):
        came = lax.rem(sp_at + sp_count - step, sp_count)
        return remote(
            final.at[step],
            result_ref.at[came],
            row_send.at[step],
            row_recv.at[step],
            came,
            tp_at,
        )

    greet(sp_count, tp_count)

    def begin(step):
        mate_copy(step).start()
        load(step).start()

    loop(1, sp_count, begin)
    begin(0)

    def add_mate(step):
        load(step).wait()
        mate_copy(step).wait_recv()
        own[step] = (
            own[step].astype(jnp.float32) + from_mate[step].astype(jnp.float32)
        ).astype(jnp.bfloat16)
        for hop in range(1, half):
            pair_copy(step, hop).start()

    loop(1, sp_count, add_mate)
    add_mate(0)

    def add_pairs(step):
        total = own[step, pair_at].astype(jnp.float32)
        for hop in range(1, half):
            pair_copy(step, hop).wait_recv()
            total = total + from_pair[step, hop - 1].astype(jnp.float32)
        final[step] = total.astype(jnp.bfloat16)

    def send_row(step):
        add_pairs(step)
        row_copy(step).start()

    loop(1, sp_count, send_row)
    add_pairs(0)
    keep = pltpu.make_async_copy(final.at[0], result_ref.at[sp_at], own_sem)
    keep.start()
    keep.wait()

    def finish(step):
        mate_copy(step).wait_send()
        for hop in range(1, half):
            pair_copy(step, hop).wait_send()

    loop(0, sp_count, finish)

    def finish_rows(step):
        row_arrival(step).wait_recv()
        row_copy(step).wait_send()

    loop(1, sp_count, finish_rows)


def bring_back(partial, collective_id):
    sp_count, half, sides, rows, width = partial.shape
    tp_count = half * sides
    sems = pltpu.SemaphoreType.DMA
    return pl.pallas_call(
        functools.partial(bring_kernel, sp_count, tp_count),
        out_shape=jax.ShapeDtypeStruct((sp_count, rows, width), partial.dtype),
        in_specs=[pl.BlockSpec(memory_space=pl.ANY)],
        out_specs=pl.BlockSpec(memory_space=pl.ANY),
        scratch_shapes=[
            pltpu.VMEM((sp_count, half, rows, width), partial.dtype),
            pltpu.VMEM((sp_count, half, rows, width), partial.dtype),
            pltpu.VMEM((sp_count, max(1, half - 1), rows, width), partial.dtype),
            pltpu.VMEM((sp_count, rows, width), partial.dtype),
            sems((sp_count,)),
            sems((sp_count,)),
            sems((sp_count,)),
            sems((sp_count, half)),
            sems((sp_count, half)),
            sems((sp_count,)),
            sems((sp_count,)),
            sems,
        ],
        compiler_params=pltpu.CompilerParams(collective_id=collective_id, has_side_effects=True),
    )(partial)


def from_behind(value, axis, steps):
    count = lax.axis_size(axis)
    initial, last = (max(0, -steps), min(count, count - steps))
    return lax.ppermute(value, axis, [(source, source + steps) for source in range(initial, last)])


def slot_choice(ids, experts, capacity):
    tokens, top_count = ids.shape
    onehots = [ids[:, k : k + 1] == jnp.arange(experts, dtype=jnp.int32)[None, :] for k in range(top_count)]
    named = sum(onehot.astype(jnp.bfloat16) for onehot in onehots)
    order = jnp.arange(tokens, dtype=jnp.int32)
    earlier = (order[None, :] < order[:, None]).astype(jnp.bfloat16)
    ranks = jnp.dot(earlier, named, preferred_element_type=jnp.float32).astype(jnp.int32)
    places = ranks + capacity * jnp.arange(experts, dtype=jnp.int32)[None, :]
    slots = jnp.arange(experts * capacity, dtype=jnp.int32)[None, :]
    return [
        (jnp.sum(jnp.where(onehot, places, 0), axis=1, keepdims=True) == slots).astype(jnp.bfloat16)
        for onehot in onehots
    ]


def expert_work(rows_in, cot_rows, gate_w, up_w, down_w):
    gate_pre = jnp.dot(rows_in, gate_w, preferred_element_type=jnp.float32)
    up_pre = jnp.dot(rows_in, up_w, preferred_element_type=jnp.float32)
    gate_sig = jax.nn.sigmoid(gate_pre)
    gate_act = gate_pre * gate_sig
    hidden = (gate_act * up_pre).astype(jnp.bfloat16)
    down_grad = lax.dot_general(
        hidden, cot_rows, (((0,), (0,)), ((), ())), preferred_element_type=jnp.float32
    )
    grad_hidden = lax.dot_general(
        cot_rows, down_w, (((1,), (1,)), ((), ())), preferred_element_type=jnp.float32
    )
    up_grad = (grad_hidden * gate_act).astype(jnp.bfloat16)
    gate_grad = (grad_hidden * up_pre * gate_sig * (1.0 + gate_pre * (1.0 - gate_sig))).astype(
        jnp.bfloat16
    )
    gate_wgrad = lax.dot_general(
        rows_in, gate_grad, (((0,), (0,)), ((), ())), preferred_element_type=jnp.float32
    )
    up_wgrad = lax.dot_general(
        rows_in, up_grad, (((0,), (0,)), ((), ())), preferred_element_type=jnp.float32
    )
    grads_pair = jnp.stack([gate_grad, up_grad], axis=1)
    weights_pair = jnp.stack([gate_w, up_w], axis=1)
    back_rows = lax.dot_general(
        grads_pair, weights_pair, (((1, 2), (1, 2)), ((), ())), preferred_element_type=jnp.float32
    ).astype(jnp.bfloat16)
    return (gate_wgrad, up_wgrad, down_grad, back_rows)


def pick(choice, rows):
    return lax.dot_general(
        choice, rows, (((0,), (0,)), ((), ())), preferred_element_type=jnp.float32
    ).astype(jnp.bfloat16)


def shards(
    stream_in,
    stream_cot,
    route_ids,
    route_wts,
    norm_gain,
    w_gate,
    w_up,
    w_down,
    out_proj,
    conv_b,
    conv_c,
    conv_h,
    conv_taps,
):
    tp_count = lax.axis_size("tp")
    sp_count = lax.axis_size("sp")
    tp_index = lax.axis_index("tp")
    tok_rows, model_width = stream_in.shape
    top_count = route_ids.shape[1]
    capacity = max(2, 5 * top_count * tok_rows // (4 * sp_count))
    inputs = stream_in.astype(jnp.float32)
    inv_rms = lax.rsqrt(jnp.mean(inputs * inputs, axis=1, keepdims=True) + epsilon)
    scaled = inputs * inv_rms
    normed = (scaled * norm_gain[None, :]).astype(jnp.bfloat16)
    own_ids = lax.dynamic_slice_in_dim(route_ids, tp_index * tok_rows, tok_rows, 0)
    own_wts = lax.dynamic_slice_in_dim(route_wts, tp_index * tok_rows, tok_rows, 0)
    choice = slot_choice(own_ids, sp_count, capacity)
    chosen = sum(choice)
    cot = stream_cot.astype(jnp.float32)
    weighted = jnp.concatenate(
        [(own_wts[:, k : k + 1] * cot).astype(jnp.bfloat16) for k in range(top_count)], axis=0
    )
    buffer_rows = pick(chosen, normed).reshape(sp_count, capacity, model_width)
    buffer_cot = pick(jnp.concatenate(choice, axis=0), weighted).reshape(
        sp_count, capacity, model_width
    )
    arrived_rows, arrived_cot = spread(sp_count, tp_count, [buffer_rows, buffer_cot], [], 1)
    gate_wgrad, up_wgrad, down_grad, back_rows = expert_work(
        arrived_rows.reshape(-1, model_width),
        arrived_cot.reshape(-1, model_width),
        w_gate[0],
        w_up[0],
        w_down[0],
    )
    returned = bring_back(
        back_rows.reshape(sp_count, tp_count // 2, 2, capacity, model_width), 2
    )
    grad_normed = jnp.dot(
        chosen,
        returned.reshape(sp_count * capacity, model_width),
        preferred_element_type=jnp.float32,
    )
    q_term = grad_normed * norm_gain[None, :]
    stream_grad = (
        stream_cot.astype(jnp.float32)
        + inv_rms * (q_term - scaled * jnp.mean(q_term * scaled, axis=1, keepdims=True))
    ).astype(jnp.bfloat16)
    feature_blocks = stream_grad.reshape(tok_rows, sp_count, -1).transpose(1, 0, 2)
    own_features, group_grad = spread(sp_count, tp_count, [feature_blocks], [stream_grad], 3)
    group_grad = group_grad.reshape(-1, model_width)
    grad_mix = lax.dot_general(
        group_grad, out_proj, (((1,), (1,)), ((), ())), preferred_element_type=jnp.float32
    ).astype(jnp.bfloat16)
    rim_prev = from_behind(jnp.stack([conv_c[-2:], conv_h[-2:]]), "sp", 1)
    gate_ext = jnp.concatenate([rim_prev[0], conv_c], axis=0).astype(jnp.float32)
    value_ext = jnp.concatenate([rim_prev[1], conv_h], axis=0).astype(jnp.float32)
    conv_in = gate_ext * value_ext
    conv_out = (
        conv_taps[0][None, :] * conv_in[:-2]
        + conv_taps[1][None, :] * conv_in[1:-1]
        + conv_taps[2][None, :] * conv_in[2:]
    )
    mixed = (conv_b.astype(jnp.float32) * conv_out).astype(jnp.bfloat16)
    all_mixed = lax.all_gather(mixed, "sp", axis=0, tiled=True)
    proj_grad = lax.dot_general(
        own_features.reshape(all_mixed.shape[0], -1),
        all_mixed,
        (((0,), (0,)), ((), ())),
        preferred_element_type=jnp.float32,
    )
    grad_b = (grad_mix.astype(jnp.float32) * conv_out).astype(jnp.bfloat16)
    rim_next = from_behind(jnp.stack([grad_mix[:2], conv_b[:2]]), "sp", -1)
    conv_grad = grad_mix.astype(jnp.float32) * conv_b.astype(jnp.float32)
    next_grad = rim_next[0].astype(jnp.float32) * rim_next[1].astype(jnp.float32)
    grad_ext = jnp.concatenate([conv_grad, next_grad], axis=0)
    grad_in = (
        conv_taps[2][None, :] * grad_ext[:-2]
        + conv_taps[1][None, :] * grad_ext[1:-1]
        + conv_taps[0][None, :] * grad_ext[2:]
    )
    grad_c = (grad_in * conv_h.astype(jnp.float32)).astype(jnp.bfloat16)
    grad_h = (grad_in * conv_c.astype(jnp.float32)).astype(jnp.bfloat16)
    return (gate_wgrad[None], up_wgrad[None], down_grad[None], proj_grad, grad_b, grad_c, grad_h)


def solution(mesh):
    in_specs = (
        P(("sp", "tp"), None),
        P(("sp", "tp"), None),
        P("sp", None),
        P("sp", None),
        P(),
        P("sp", None, "tp"),
        P("sp", None, "tp"),
        P("sp", "tp", None),
        P("tp", None),
        P("sp", "tp"),
        P("sp", "tp"),
        P("sp", "tp"),
        P(None, "tp"),
    )
    out_specs = (
        P("sp", None, "tp"),
        P("sp", None, "tp"),
        P("sp", "tp", None),
        P("sp", "tp"),
        P("sp", "tp"),
        P("sp", "tp"),
        P("sp", "tp"),
    )
    return jax.shard_map(shards, mesh=mesh, in_specs=in_specs, out_specs=out_specs, check_vma=False)
```

```python
import functools

import jax
import jax.numpy as jnp
from jax import lax
from jax.experimental import pallas as pl
from jax.experimental.pallas import tpu as pltpu
from jax.sharding import PartitionSpec as P

epsilon = 1e-06


def here():
    return lax.axis_index("sp"), lax.axis_index("tp")


def greet(sp_count, tp_count):
    sp_at, tp_at = here()
    half = tp_count // 2
    barrier = pltpu.get_barrier_semaphore()

    def hail(sp_to, tp_to):
        pl.semaphore_signal(
            barrier, inc=1, device_id=(sp_to, tp_to), device_id_type=pl.DeviceIdType.MESH
        )

    def hail_row(step, carry):
        hail(lax.rem(sp_at + step, sp_count), tp_at)
        return carry

    lax.fori_loop(1, sp_count, hail_row, 0)
    for step in range(1, half):
        hail(sp_at, pair_peer(tp_at, step, half))
    hail(sp_at, mate_of(tp_at))
    pl.semaphore_wait(barrier, sp_count - 1 + half)


def pair_peer(tp_at, step, half):
    return lax.rem(tp_at // 2 + step, half) * 2 + lax.rem(tp_at, 2)


def mate_of(tp_at):
    return tp_at + 1 - 2 * lax.rem(tp_at, 2)


def remote(source, target, send_sem, recv_sem, sp_to, tp_to):
    return pltpu.make_async_remote_copy(
        src_ref=source,
        dst_ref=target,
        send_sem=send_sem,
        recv_sem=recv_sem,
        device_id=(sp_to, tp_to),
        device_id_type=pl.DeviceIdType.MESH,
    )


def loop(first, last, body):
    def step(index, carry):
        body(index)
        return carry

    lax.fori_loop(first, last, step, 0)


def spread_kernel(sp_count, tp_count, exchanged, gathered, shifted, lined, edged, *refs):
    count = exchanged + gathered
    moved = len(shifted)
    total = count + moved + lined
    sources, results = refs[:count], refs[total : total + count]
    shift_sources, shift_results = refs[count : count + moved], refs[total + count : total + count + moved]
    line_source = refs[total - 1]
    line_result = refs[2 * total - 1]
    edge_result = refs[2 * total]
    (
        own_sem,
        row_send,
        row_recv,
        pair_send,
        pair_recv,
        mate_send,
        mate_recv,
        last_send,
        last_recv,
        shift_send,
        shift_recv,
        line_send,
        line_recv,
        edge_sem,
    ) = refs[2 * total + edged :]
    sp_at, tp_at = here()
    half = tp_count // 2
    mate = mate_of(tp_at)

    def origin(step):
        return lax.rem(sp_at + sp_count - step, sp_count)

    def slot_of(which, step, tp_from):
        if which < exchanged:
            return results[which].at[origin(step), tp_from]
        return results[which].at[tp_from]

    def own_block(which):
        return sources[which].at[sp_at] if which < exchanged else sources[which]

    def row_copy(which, step):
        to = lax.rem(sp_at + step, sp_count)
        return remote(
            sources[which].at[to],
            results[which].at[sp_at, tp_at],
            row_send.at[which, step],
            row_recv.at[which, step],
            to,
            tp_at,
        )

    def row_arrival(which, step):
        return remote(
            own_block(which),
            slot_of(which, step, tp_at),
            row_send.at[which, step],
            row_recv.at[which, step],
            origin(step),
            tp_at,
        )

    def pair_copy(which, step, hop, source, tp_from):
        return remote(
            source,
            slot_of(which, step, tp_from),
            pair_send.at[which, step, hop],
            pair_recv.at[which, step, hop],
            sp_at,
            pair_peer(tp_at, hop, half),
        )

    def mate_copy(which, step, source, tp_from):
        return remote(
            source,
            slot_of(which, step, tp_from),
            mate_send.at[which, step],
            mate_recv.at[which, step],
            sp_at,
            mate,
        )

    def last_copy(which, step, hop, tp_from):
        return remote(
            slot_of(which, step, tp_from),
            slot_of(which, step, tp_from),
            last_send.at[which, step, hop],
            last_recv.at[which, step, hop],
            sp_at,
            mate,
        )

    def pair_source(hop):
        return pair_peer(tp_at, half - hop, half)

    def pass_on(which, step, source):
        for hop in range(1, half):
            pair_copy(which, step, hop, source, tp_at).start()
        mate_copy(which, step, source, tp_at).start()

    def pass_last(which, step):
        for hop in range(1, half):
            origin_tp = pair_source(hop)
            pair_copy(which, step, hop, own_block(which), origin_tp).wait_recv()
            last_copy(which, step, hop, origin_tp).start()

    def shift_copy(index):
        to = lax.rem(sp_at + sp_count + shifted[index], sp_count)
        return remote(
            shift_sources[index],
            shift_results[index],
            shift_send.at[index],
            shift_recv.at[index],
            to,
            tp_at,
        )

    edge_rows = edge_result.shape[0] if edged else 0

    def edge_copy():
        return remote(
            results[exchanged].at[0, pl.ds(0, edge_rows)],
            edge_result,
            edge_sem.at[0],
            edge_sem.at[1],
            origin(1),
            tp_at,
        )

    depth = sp_count // 2
    deep, lane = sp_at // 2, lax.rem(sp_at, 2)

    def line_slot(where, side):
        return line_result.at[where * 2 + side]

    def line_copy(way, step):
        toward = 1 - 2 * way
        where = jnp.clip(deep - toward * step, 0, depth - 1)
        return remote(
            line_slot(where, lane),
            line_slot(where, lane),
            line_send.at[way, step],
            line_recv.at[way, step + 1],
            jnp.clip(deep + toward, 0, depth - 1) * 2 + lane,
            tp_at,
        )

    def line_arrival(way, step):
        toward = 1 - 2 * way
        where = jnp.clip(deep - toward * step, 0, depth - 1)
        return remote(
            line_slot(where, lane),
            line_slot(where, lane),
            line_send.at[way, step],
            line_recv.at[way, step],
            jnp.clip(deep - toward, 0, depth - 1) * 2 + lane,
            tp_at,
        )

    def line_mate(where, side):
        return remote(
            line_slot(where, side),
            line_slot(where, side),
            line_send.at[2, where],
            line_recv.at[2, where],
            deep * 2 + 1 - lane,
            tp_at,
        )

    def reach(way):
        return deep if way == 0 else depth - 1 - deep

    def line_pass(way, step):
        @pl.when(reach(1 - way) > 0)
        def _():
            line_copy(way, step).start()

    def line_step(step):
        for way in range(2):

            @pl.when(step <= reach(way))
            def _():
                line_arrival(way, step).wait_recv()
                line_pass(way, step)
                toward = 1 - 2 * way
                line_mate(jnp.clip(deep - toward * step, 0, depth - 1), lane).start()

    greet(sp_count, tp_count)
    for index in range(moved):
        shift_copy(index).start()
    if lined:
        line_own = pltpu.make_async_copy(line_source, line_slot(deep, lane), edge_sem.at[2])
        line_own.start()
    for which in range(exchanged):
        loop(1, sp_count, lambda step: row_copy(which, step).start())
    locals_ = [
        pltpu.make_async_copy(own_block(which), slot_of(which, 0, tp_at), own_sem.at[which])
        for which in range(count)
    ]
    for copy in locals_:
        copy.start()
    for which in reversed(range(count)):
        pass_on(which, 0, own_block(which))

    if lined:
        line_own.wait()
        for way in range(2):
            line_pass(way, 0)
        line_mate(deep, lane).start()
    for which in range(exchanged, count):
        pass_last(which, 0)
    for which in range(exchanged):

        def relay(step):
            row_arrival(which, step).wait_recv()
            pass_on(which, step, slot_of(which, step, tp_at))
            pass_last(which, step - 1)
            if lined and which == 0:

                @pl.when(lax.rem(step, 2) == 0)
                def _():
                    line_step(step // 2)

        loop(1, sp_count, relay)
        pass_last(which, sp_count - 1)

    for copy in locals_:
        copy.wait()
    for which in reversed(range(count)):
        steps = sp_count if which < exchanged else 1

        def finish(step):
            for hop in range(1, half):
                pair_copy(which, step, hop, own_block(which), tp_at).wait_send()
                last_copy(which, step, hop, pair_source(hop)).wait_send()
                last_copy(
                    which, step, hop, mate_of(pair_source(hop))
                ).wait_recv()
            mate_copy(which, step, own_block(which), tp_at).wait_send()
            mate_copy(which, step, own_block(which), mate).wait_recv()

        loop(0, steps, finish)
        if which < exchanged:
            loop(1, sp_count, lambda step: row_copy(which, step).wait_send())
        elif edged and which == exchanged:
            edge_copy().start()

    for index in range(moved):
        shift_copy(index).wait()
    if lined:
        for way in range(2):

            @pl.when(reach(1 - way) > 0)
            def _():
                loop(0, reach(way) + 1, lambda step: line_copy(way, step).wait_send())

        def finish_line(where):
            line_mate(where, lane).wait_send()
            line_mate(where, 1 - lane).wait_recv()

        loop(0, depth, finish_line)
    if edged:
        edge_copy().wait()


def spread(sp_count, tp_count, exchanged, gathered, shifted, lined, edge_rows, collective_id):
    arrays = exchanged + gathered + [value for value, _ in shifted] + lined
    count = len(exchanged) + len(gathered)
    half = tp_count // 2
    edged = 1 if edge_rows else 0
    shapes = (
        [(sp_count, tp_count) + value.shape[1:] for value in exchanged]
        + [(tp_count,) + value.shape for value in gathered]
        + [value.shape for value, _ in shifted]
        + [(sp_count,) + value.shape for value in lined]
    )
    out_shape = [
        jax.ShapeDtypeStruct(shape, value.dtype) for shape, value in zip(shapes, arrays)
    ]
    if edged:
        out_shape.append(
            jax.ShapeDtypeStruct((edge_rows, gathered[0].shape[1]), gathered[0].dtype)
        )
    sems = pltpu.SemaphoreType.DMA
    return pl.pallas_call(
        functools.partial(
            spread_kernel,
            sp_count,
            tp_count,
            len(exchanged),
            len(gathered),
            tuple(step for _, step in shifted),
            len(lined),
            edged,
        ),
        out_shape=tuple(out_shape),
        in_specs=[pl.BlockSpec(memory_space=pltpu.VMEM)] * len(arrays),
        out_specs=tuple([pl.BlockSpec(memory_space=pl.ANY)] * len(out_shape)),
        scratch_shapes=[sems((count,))]
        + [sems((count, sp_count))] * 2
        + [sems((count, sp_count, half))] * 2
        + [sems((count, sp_count))] * 2
        + [sems((count, sp_count, half))] * 2
        + [sems((max(1, len(shifted)),))] * 2
        + [sems((3, sp_count // 2 + 1))] * 2
        + [sems((3,))],
        compiler_params=pltpu.CompilerParams(collective_id=collective_id, has_side_effects=True),
    )(*arrays)


def bring_kernel(
    sp_count,
    tp_count,
    partial_ref,
    result_ref,
    own,
    from_mate,
    from_pair,
    final,
    load_sem,
    mate_send,
    mate_recv,
    pair_send,
    pair_recv,
    row_send,
    row_recv,
    own_sem,
):
    sp_at, tp_at = here()
    half = tp_count // 2
    pair_at, side = tp_at // 2, lax.rem(tp_at, 2)
    mate = mate_of(tp_at)

    def target(step):
        return lax.rem(sp_at + step, sp_count)

    def load(step):
        return pltpu.make_async_copy(
            partial_ref.at[target(step), :, side], own.at[step], load_sem.at[step]
        )

    def mate_copy(step):
        return remote(
            partial_ref.at[target(step), :, 1 - side],
            from_mate.at[step],
            mate_send.at[step],
            mate_recv.at[step],
            sp_at,
            mate,
        )

    def pair_copy(step, hop):
        return remote(
            own.at[step, lax.rem(pair_at + hop, half)],
            from_pair.at[step, hop - 1],
            pair_send.at[step, hop],
            pair_recv.at[step, hop],
            sp_at,
            pair_peer(tp_at, hop, half),
        )

    def row_copy(step):
        return remote(
            final.at[step],
            result_ref.at[sp_at],
            row_send.at[step],
            row_recv.at[step],
            target(step),
            tp_at,
        )

    def row_arrival(step):
        came = lax.rem(sp_at + sp_count - step, sp_count)
        return remote(
            final.at[step],
            result_ref.at[came],
            row_send.at[step],
            row_recv.at[step],
            came,
            tp_at,
        )

    greet(sp_count, tp_count)

    def begin(step):
        mate_copy(step).start()
        load(step).start()

    loop(1, sp_count, begin)
    begin(0)

    def add_mate(step):
        load(step).wait()
        mate_copy(step).wait_recv()
        own[step] = (
            own[step].astype(jnp.float32) + from_mate[step].astype(jnp.float32)
        ).astype(jnp.bfloat16)
        for hop in range(1, half):
            pair_copy(step, hop).start()

    loop(1, sp_count, add_mate)
    add_mate(0)

    def add_pairs(step):
        total = own[step, pair_at].astype(jnp.float32)
        for hop in range(1, half):
            pair_copy(step, hop).wait_recv()
            total = total + from_pair[step, hop - 1].astype(jnp.float32)
        final[step] = total.astype(jnp.bfloat16)

    def send_row(step):
        add_pairs(step)
        row_copy(step).start()

    loop(1, sp_count, send_row)
    add_pairs(0)
    keep = pltpu.make_async_copy(final.at[0], result_ref.at[sp_at], own_sem)
    keep.start()
    keep.wait()

    def finish(step):
        mate_copy(step).wait_send()
        for hop in range(1, half):
            pair_copy(step, hop).wait_send()

    loop(0, sp_count, finish)

    def finish_rows(step):
        row_arrival(step).wait_recv()
        row_copy(step).wait_send()

    loop(1, sp_count, finish_rows)


def bring_back(partial, collective_id):
    sp_count, half, sides, rows, width = partial.shape
    tp_count = half * sides
    sems = pltpu.SemaphoreType.DMA
    return pl.pallas_call(
        functools.partial(bring_kernel, sp_count, tp_count),
        out_shape=jax.ShapeDtypeStruct((sp_count, rows, width), partial.dtype),
        in_specs=[pl.BlockSpec(memory_space=pl.ANY)],
        out_specs=pl.BlockSpec(memory_space=pl.ANY),
        scratch_shapes=[
            pltpu.VMEM((sp_count, half, rows, width), partial.dtype),
            pltpu.VMEM((sp_count, half, rows, width), partial.dtype),
            pltpu.VMEM((sp_count, max(1, half - 1), rows, width), partial.dtype),
            pltpu.VMEM((sp_count, rows, width), partial.dtype),
            sems((sp_count,)),
            sems((sp_count,)),
            sems((sp_count,)),
            sems((sp_count, half)),
            sems((sp_count, half)),
            sems((sp_count,)),
            sems((sp_count,)),
            sems,
        ],
        compiler_params=pltpu.CompilerParams(collective_id=collective_id, has_side_effects=True),
    )(partial)


def slot_choice(ids, experts, capacity):
    tokens, top_count = ids.shape
    onehots = [ids[:, k : k + 1] == jnp.arange(experts, dtype=jnp.int32)[None, :] for k in range(top_count)]
    named = sum(onehot.astype(jnp.bfloat16) for onehot in onehots)
    order = jnp.arange(tokens, dtype=jnp.int32)
    earlier = (order[None, :] < order[:, None]).astype(jnp.bfloat16)
    ranks = jnp.dot(earlier, named, preferred_element_type=jnp.float32).astype(jnp.int32)
    places = ranks + capacity * jnp.arange(experts, dtype=jnp.int32)[None, :]
    slots = jnp.arange(experts * capacity, dtype=jnp.int32)[None, :]
    return [
        (jnp.sum(jnp.where(onehot, places, 0), axis=1, keepdims=True) == slots).astype(jnp.bfloat16)
        for onehot in onehots
    ]


def expert_work(rows_in, cot_rows, gate_w, up_w, down_w):
    gate_pre = jnp.dot(rows_in, gate_w, preferred_element_type=jnp.float32)
    up_pre = jnp.dot(rows_in, up_w, preferred_element_type=jnp.float32)
    gate_sig = jax.nn.sigmoid(gate_pre)
    gate_act = gate_pre * gate_sig
    hidden = (gate_act * up_pre).astype(jnp.bfloat16)
    down_grad = lax.dot_general(
        hidden, cot_rows, (((0,), (0,)), ((), ())), preferred_element_type=jnp.float32
    )
    grad_hidden = lax.dot_general(
        cot_rows, down_w, (((1,), (1,)), ((), ())), preferred_element_type=jnp.float32
    )
    up_grad = (grad_hidden * gate_act).astype(jnp.bfloat16)
    gate_grad = (grad_hidden * up_pre * gate_sig * (1.0 + gate_pre * (1.0 - gate_sig))).astype(
        jnp.bfloat16
    )
    gate_wgrad = lax.dot_general(
        rows_in, gate_grad, (((0,), (0,)), ((), ())), preferred_element_type=jnp.float32
    )
    up_wgrad = lax.dot_general(
        rows_in, up_grad, (((0,), (0,)), ((), ())), preferred_element_type=jnp.float32
    )
    grads_pair = jnp.stack([gate_grad, up_grad], axis=1)
    weights_pair = jnp.stack([gate_w, up_w], axis=1)
    back_rows = lax.dot_general(
        grads_pair, weights_pair, (((1, 2), (1, 2)), ((), ())), preferred_element_type=jnp.float32
    ).astype(jnp.bfloat16)
    return (gate_wgrad, up_wgrad, down_grad, back_rows)


def pick(choice, rows):
    return lax.dot_general(
        choice, rows, (((0,), (0,)), ((), ())), preferred_element_type=jnp.float32
    ).astype(jnp.bfloat16)


def shards(
    stream_in,
    stream_cot,
    route_ids,
    route_wts,
    norm_gain,
    w_gate,
    w_up,
    w_down,
    out_proj,
    conv_b,
    conv_c,
    conv_h,
    conv_taps,
):
    tp_count = lax.axis_size("tp")
    sp_count = lax.axis_size("sp")
    tp_index = lax.axis_index("tp")
    tok_rows, model_width = stream_in.shape
    top_count = route_ids.shape[1]
    capacity = max(2, 5 * top_count * tok_rows // (4 * sp_count))
    inputs = stream_in.astype(jnp.float32)
    inv_rms = lax.rsqrt(jnp.mean(inputs * inputs, axis=1, keepdims=True) + epsilon)
    scaled = inputs * inv_rms
    normed = (scaled * norm_gain[None, :]).astype(jnp.bfloat16)
    own_ids = lax.dynamic_slice_in_dim(route_ids, tp_index * tok_rows, tok_rows, 0)
    own_wts = lax.dynamic_slice_in_dim(route_wts, tp_index * tok_rows, tok_rows, 0)
    choice = slot_choice(own_ids, sp_count, capacity)
    chosen = sum(choice)
    cot = stream_cot.astype(jnp.float32)
    weighted = jnp.concatenate(
        [(own_wts[:, k : k + 1] * cot).astype(jnp.bfloat16) for k in range(top_count)], axis=0
    )
    buffer_rows = pick(chosen, normed).reshape(sp_count, capacity, model_width)
    buffer_cot = pick(jnp.concatenate(choice, axis=0), weighted).reshape(
        sp_count, capacity, model_width
    )
    edge_rows = 8
    arrived_rows, arrived_cot, c_before, h_before, b_after = spread(
        sp_count,
        tp_count,
        [buffer_rows, buffer_cot],
        [],
        [(conv_c[-edge_rows:], 1), (conv_h[-edge_rows:], 1), (conv_b[:edge_rows], -1)],
        [],
        0,
        1,
    )
    gate_wgrad, up_wgrad, down_grad, back_rows = expert_work(
        arrived_rows.reshape(-1, model_width),
        arrived_cot.reshape(-1, model_width),
        w_gate[0],
        w_up[0],
        w_down[0],
    )
    returned = bring_back(
        back_rows.reshape(sp_count, tp_count // 2, 2, capacity, model_width), 2
    )
    grad_normed = jnp.dot(
        chosen,
        returned.reshape(sp_count * capacity, model_width),
        preferred_element_type=jnp.float32,
    )
    q_term = grad_normed * norm_gain[None, :]
    stream_grad = (
        stream_cot.astype(jnp.float32)
        + inv_rms * (q_term - scaled * jnp.mean(q_term * scaled, axis=1, keepdims=True))
    ).astype(jnp.bfloat16)
    feature_blocks = stream_grad.reshape(tok_rows, sp_count, -1).transpose(1, 0, 2)
    rim = conv_taps.shape[0] - 1
    has_before = lax.axis_index("sp") > 0
    gate_ext = jnp.concatenate([c_before[-rim:], conv_c], axis=0).astype(jnp.float32)
    value_ext = jnp.concatenate([h_before[-rim:], conv_h], axis=0).astype(jnp.float32)
    inside = has_before | (jnp.arange(gate_ext.shape[0])[:, None] >= rim)
    conv_in = jnp.where(inside, gate_ext * value_ext, 0.0)
    conv_out = (
        conv_taps[0][None, :] * conv_in[:-2]
        + conv_taps[1][None, :] * conv_in[1:-1]
        + conv_taps[2][None, :] * conv_in[2:]
    )
    mixed = (conv_b.astype(jnp.float32) * conv_out).astype(jnp.bfloat16)
    own_features, group_grad, all_mixed, edge_grad = spread(
        sp_count, tp_count, [feature_blocks], [stream_grad], [], [mixed], edge_rows, 3
    )
    group_grad = group_grad.reshape(-1, model_width)
    grad_mix = lax.dot_general(
        group_grad, out_proj, (((1,), (1,)), ((), ())), preferred_element_type=jnp.float32
    ).astype(jnp.bfloat16)
    all_mixed = all_mixed.reshape(-1, all_mixed.shape[-1])
    proj_grad = lax.dot_general(
        own_features.reshape(all_mixed.shape[0], -1),
        all_mixed,
        (((0,), (0,)), ((), ())),
        preferred_element_type=jnp.float32,
    )
    grad_b = (grad_mix.astype(jnp.float32) * conv_out).astype(jnp.bfloat16)
    edge_mix = lax.dot_general(
        edge_grad, out_proj, (((1,), (1,)), ((), ())), preferred_element_type=jnp.float32
    ).astype(jnp.bfloat16)
    conv_grad = grad_mix.astype(jnp.float32) * conv_b.astype(jnp.float32)
    next_grad = edge_mix.astype(jnp.float32) * b_after.astype(jnp.float32)
    has_after = lax.axis_index("sp") < sp_count - 1
    next_grad = jnp.where(has_after, next_grad, 0.0)[:rim]
    grad_ext = jnp.concatenate([conv_grad, next_grad], axis=0)
    grad_in = (
        conv_taps[2][None, :] * grad_ext[:-2]
        + conv_taps[1][None, :] * grad_ext[1:-1]
        + conv_taps[0][None, :] * grad_ext[2:]
    )
    grad_c = (grad_in * conv_h.astype(jnp.float32)).astype(jnp.bfloat16)
    grad_h = (grad_in * conv_c.astype(jnp.float32)).astype(jnp.bfloat16)
    return (gate_wgrad[None], up_wgrad[None], down_grad[None], proj_grad, grad_b, grad_c, grad_h)


def solution(mesh):
    in_specs = (
        P(("sp", "tp"), None),
        P(("sp", "tp"), None),
        P("sp", None),
        P("sp", None),
        P(),
        P("sp", None, "tp"),
        P("sp", None, "tp"),
        P("sp", "tp", None),
        P("tp", None),
        P("sp", "tp"),
        P("sp", "tp"),
        P("sp", "tp"),
        P(None, "tp"),
    )
    out_specs = (
        P("sp", None, "tp"),
        P("sp", None, "tp"),
        P("sp", "tp", None),
        P("sp", "tp"),
        P("sp", "tp"),
        P("sp", "tp"),
        P("sp", "tp"),
    )
    return jax.shard_map(shards, mesh=mesh, in_specs=in_specs, out_specs=out_specs, check_vma=False)
```

```python
import functools

import jax
import jax.numpy as jnp
from jax import lax
from jax.experimental import pallas as pl
from jax.experimental.pallas import tpu as pltpu
from jax.sharding import PartitionSpec as P

epsilon = 1e-06


def here():
    return lax.axis_index("sp"), lax.axis_index("tp")


def greet(sp_count, tp_count):
    sp_at, tp_at = here()
    half = tp_count // 2
    barrier = pltpu.get_barrier_semaphore()

    def hail(sp_to, tp_to):
        pl.semaphore_signal(
            barrier, inc=1, device_id=(sp_to, tp_to), device_id_type=pl.DeviceIdType.MESH
        )

    def hail_row(step, carry):
        hail(lax.rem(sp_at + step, sp_count), tp_at)
        return carry

    lax.fori_loop(1, sp_count, hail_row, 0)
    for step in range(1, half):
        hail(sp_at, pair_peer(tp_at, step, half))
    hail(sp_at, mate_of(tp_at))
    pl.semaphore_wait(barrier, sp_count - 1 + half)


def pair_peer(tp_at, step, half):
    return lax.rem(tp_at // 2 + step, half) * 2 + lax.rem(tp_at, 2)


def partner(at, step, count):
    other = lax.rem(count - step, count)
    total, bit = 0, 1
    while bit < count:
        total = total + bit * lax.rem(at // bit + other // bit, 2)
        bit *= 2
    return total


def mate_of(tp_at):
    return tp_at + 1 - 2 * lax.rem(tp_at, 2)


def remote(source, target, send_sem, recv_sem, sp_to, tp_to):
    return pltpu.make_async_remote_copy(
        src_ref=source,
        dst_ref=target,
        send_sem=send_sem,
        recv_sem=recv_sem,
        device_id=(sp_to, tp_to),
        device_id_type=pl.DeviceIdType.MESH,
    )


def loop(first, last, body):
    def step(index, carry):
        body(index)
        return carry

    lax.fori_loop(first, last, step, 0)


def spread_kernel(sp_count, tp_count, exchanged, gathered, shifted, lined, edged, *refs):
    count = exchanged + gathered
    moved = len(shifted)
    total = count + moved + lined
    sources, results = refs[:count], refs[total : total + count]
    shift_sources, shift_results = refs[count : count + moved], refs[total + count : total + count + moved]
    line_source = refs[total - 1]
    line_result = refs[2 * total - 1]
    edge_result = refs[2 * total]
    (
        own_sem,
        row_send,
        row_recv,
        pair_send,
        pair_recv,
        mate_send,
        mate_recv,
        last_send,
        last_recv,
        shift_send,
        shift_recv,
        line_send,
        line_recv,
        edge_sem,
    ) = refs[2 * total + edged :]
    sp_at, tp_at = here()
    half = tp_count // 2
    mate = mate_of(tp_at)

    def origin(step):
        return partner(sp_at, step, sp_count)

    def slot_of(which, step, tp_from):
        if which < exchanged:
            return results[which].at[origin(step), tp_from]
        return results[which].at[tp_from]

    def own_block(which):
        return sources[which].at[sp_at] if which < exchanged else sources[which]

    def row_copy(which, step):
        to = origin(step)
        return remote(
            sources[which].at[to],
            results[which].at[sp_at, tp_at],
            row_send.at[which, step],
            row_recv.at[which, step],
            to,
            tp_at,
        )

    def row_arrival(which, step):
        return remote(
            own_block(which),
            slot_of(which, step, tp_at),
            row_send.at[which, step],
            row_recv.at[which, step],
            origin(step),
            tp_at,
        )

    def pair_copy(which, step, hop, source, tp_from):
        return remote(
            source,
            slot_of(which, step, tp_from),
            pair_send.at[which, step, hop],
            pair_recv.at[which, step, hop],
            sp_at,
            pair_peer(tp_at, hop, half),
        )

    def mate_copy(which, step, source, tp_from):
        return remote(
            source,
            slot_of(which, step, tp_from),
            mate_send.at[which, step],
            mate_recv.at[which, step],
            sp_at,
            mate,
        )

    def last_copy(which, step, hop, tp_from):
        return remote(
            slot_of(which, step, tp_from),
            slot_of(which, step, tp_from),
            last_send.at[which, step, hop],
            last_recv.at[which, step, hop],
            sp_at,
            mate,
        )

    def pair_source(hop):
        return pair_peer(tp_at, half - hop, half)

    def pass_on(which, step, source):
        for hop in range(1, half):
            pair_copy(which, step, hop, source, tp_at).start()
        mate_copy(which, step, source, tp_at).start()

    def pass_last(which, step):
        for hop in range(1, half):
            origin_tp = pair_source(hop)
            pair_copy(which, step, hop, own_block(which), origin_tp).wait_recv()
            last_copy(which, step, hop, origin_tp).start()

    def shift_copy(index):
        to = lax.rem(sp_at + sp_count + shifted[index], sp_count)
        rows = shift_results[index].shape[0]
        first = shift_sources[index].shape[0] - rows if shifted[index] > 0 else 0
        return remote(
            shift_sources[index].at[pl.ds(first, rows)],
            shift_results[index],
            shift_send.at[index],
            shift_recv.at[index],
            to,
            tp_at,
        )

    edge_rows = edge_result.shape[0] if edged else 0

    def edge_copy():
        return remote(
            results[exchanged].at[0, pl.ds(0, edge_rows)],
            edge_result,
            edge_sem.at[0],
            edge_sem.at[1],
            lax.rem(sp_at + sp_count - 1, sp_count),
            tp_at,
        )

    depth = sp_count // 2
    deep, lane = sp_at // 2, lax.rem(sp_at, 2)

    def line_slot(where, side):
        return line_result.at[where * 2 + side]

    def line_copy(way, step):
        toward = 1 - 2 * way
        where = jnp.clip(deep - toward * step, 0, depth - 1)
        return remote(
            line_slot(where, lane),
            line_slot(where, lane),
            line_send.at[way, step],
            line_recv.at[way, step + 1],
            jnp.clip(deep + toward, 0, depth - 1) * 2 + lane,
            tp_at,
        )

    def line_arrival(way, step):
        toward = 1 - 2 * way
        where = jnp.clip(deep - toward * step, 0, depth - 1)
        return remote(
            line_slot(where, lane),
            line_slot(where, lane),
            line_send.at[way, step],
            line_recv.at[way, step],
            jnp.clip(deep - toward, 0, depth - 1) * 2 + lane,
            tp_at,
        )

    def line_mate(where, side):
        return remote(
            line_slot(where, side),
            line_slot(where, side),
            line_send.at[2, where],
            line_recv.at[2, where],
            deep * 2 + 1 - lane,
            tp_at,
        )

    def reach(way):
        return deep if way == 0 else depth - 1 - deep

    def line_pass(way, step):
        @pl.when(reach(1 - way) > 0)
        def _():
            line_copy(way, step).start()

    def line_step(step):
        for way in range(2):

            @pl.when(step <= reach(way))
            def _():
                line_arrival(way, step).wait_recv()
                line_pass(way, step)
                toward = 1 - 2 * way
                line_mate(jnp.clip(deep - toward * step, 0, depth - 1), lane).start()

    greet(sp_count, tp_count)
    for index in range(moved):
        shift_copy(index).start()
    if lined:
        line_own = pltpu.make_async_copy(line_source, line_slot(deep, lane), edge_sem.at[2])
        line_own.start()
    for which in range(exchanged):
        loop(1, sp_count, lambda step: row_copy(which, step).start())
    locals_ = [
        pltpu.make_async_copy(own_block(which), slot_of(which, 0, tp_at), own_sem.at[which])
        for which in range(count)
    ]
    for copy in locals_:
        copy.start()
    for which in reversed(range(count)):
        pass_on(which, 0, own_block(which))

    if lined:
        line_own.wait()
        for way in range(2):
            line_pass(way, 0)
        line_mate(deep, lane).start()
    for which in range(exchanged, count):
        pass_last(which, 0)
    for which in range(exchanged):

        def step_at(place):
            return lax.rem(place + sp_count - 3, sp_count - 1) + 1

        def relay(step, before):
            row_arrival(which, step).wait_recv()
            pass_on(which, step, slot_of(which, step, tp_at))
            pass_last(which, before)

        def relay_at(place):
            relay(step_at(place), step_at(place - 1))
            if lined and which == 0:

                @pl.when(lax.rem(place, 2) == 0)
                def _():
                    line_step(place // 2)

        relay(sp_count - 1, 0)
        loop(2, sp_count, relay_at)
        pass_last(which, sp_count - 2)

    for copy in locals_:
        copy.wait()
    for which in reversed(range(count)):
        steps = sp_count if which < exchanged else 1

        def finish(step):
            for hop in range(1, half):
                pair_copy(which, step, hop, own_block(which), tp_at).wait_send()
                last_copy(which, step, hop, pair_source(hop)).wait_send()
                last_copy(
                    which, step, hop, mate_of(pair_source(hop))
                ).wait_recv()
            mate_copy(which, step, own_block(which), tp_at).wait_send()
            mate_copy(which, step, own_block(which), mate).wait_recv()

        loop(0, steps, finish)
        if which < exchanged:
            loop(1, sp_count, lambda step: row_copy(which, step).wait_send())
        elif edged and which == exchanged:
            edge_copy().start()

    for index in range(moved):
        shift_copy(index).wait()
    if lined:
        for way in range(2):

            @pl.when(reach(1 - way) > 0)
            def _():
                loop(0, reach(way) + 1, lambda step: line_copy(way, step).wait_send())

        def finish_line(where):
            line_mate(where, lane).wait_send()
            line_mate(where, 1 - lane).wait_recv()

        loop(0, depth, finish_line)
    if edged:
        edge_copy().wait()


def spread(sp_count, tp_count, exchanged, gathered, shifted, lined, edge_rows, collective_id):
    arrays = exchanged + gathered + [value for value, _ in shifted] + lined
    count = len(exchanged) + len(gathered)
    half = tp_count // 2
    edged = 1 if edge_rows and gathered else 0
    shapes = (
        [(sp_count, tp_count) + value.shape[1:] for value in exchanged]
        + [(tp_count,) + value.shape for value in gathered]
        + [(edge_rows,) + value.shape[1:] for value, _ in shifted]
        + [(sp_count,) + value.shape for value in lined]
    )
    out_shape = [
        jax.ShapeDtypeStruct(shape, value.dtype) for shape, value in zip(shapes, arrays)
    ]
    if edged:
        out_shape.append(
            jax.ShapeDtypeStruct((edge_rows, gathered[0].shape[1]), gathered[0].dtype)
        )
    sems = pltpu.SemaphoreType.DMA
    return pl.pallas_call(
        functools.partial(
            spread_kernel,
            sp_count,
            tp_count,
            len(exchanged),
            len(gathered),
            tuple(step for _, step in shifted),
            len(lined),
            edged,
        ),
        out_shape=tuple(out_shape),
        in_specs=[pl.BlockSpec(memory_space=pltpu.VMEM)] * count
        + [pl.BlockSpec(memory_space=pl.ANY)] * len(shifted)
        + [pl.BlockSpec(memory_space=pltpu.VMEM)] * len(lined),
        out_specs=tuple([pl.BlockSpec(memory_space=pl.ANY)] * len(out_shape)),
        scratch_shapes=[sems((count,))]
        + [sems((count, sp_count))] * 2
        + [sems((count, sp_count, half))] * 2
        + [sems((count, sp_count))] * 2
        + [sems((count, sp_count, half))] * 2
        + [sems((max(1, len(shifted)),))] * 2
        + [sems((3, sp_count // 2 + 1))] * 2
        + [sems((3,))],
        compiler_params=pltpu.CompilerParams(collective_id=collective_id, has_side_effects=True),
    )(*arrays)


def bring_kernel(
    sp_count,
    tp_count,
    partial_ref,
    result_ref,
    own,
    from_mate,
    from_pair,
    final,
    load_sem,
    mate_send,
    mate_recv,
    pair_send,
    pair_recv,
    row_send,
    row_recv,
    own_sem,
):
    sp_at, tp_at = here()
    half = tp_count // 2
    pair_at, side = tp_at // 2, lax.rem(tp_at, 2)
    mate = mate_of(tp_at)

    def target(step):
        return partner(sp_at, step, sp_count)

    def load(step):
        return pltpu.make_async_copy(
            partial_ref.at[target(step), :, side], own.at[step], load_sem.at[step]
        )

    def mate_copy(step):
        return remote(
            partial_ref.at[target(step), :, 1 - side],
            from_mate.at[step],
            mate_send.at[step],
            mate_recv.at[step],
            sp_at,
            mate,
        )

    def pair_copy(step, hop):
        return remote(
            own.at[step, lax.rem(pair_at + hop, half)],
            from_pair.at[step, hop - 1],
            pair_send.at[step, hop],
            pair_recv.at[step, hop],
            sp_at,
            pair_peer(tp_at, hop, half),
        )

    def row_copy(step):
        return remote(
            final.at[step],
            result_ref.at[sp_at],
            row_send.at[step],
            row_recv.at[step],
            target(step),
            tp_at,
        )

    def row_arrival(step):
        came = target(step)
        return remote(
            final.at[step],
            result_ref.at[came],
            row_send.at[step],
            row_recv.at[step],
            came,
            tp_at,
        )

    greet(sp_count, tp_count)

    def begin(step):
        mate_copy(step).start()
        load(step).start()

    loop(1, sp_count, begin)
    begin(0)

    def add_mate(step):
        load(step).wait()
        mate_copy(step).wait_recv()
        own[step] = (
            own[step].astype(jnp.float32) + from_mate[step].astype(jnp.float32)
        ).astype(jnp.bfloat16)
        for hop in range(1, half):
            pair_copy(step, hop).start()

    loop(1, sp_count, add_mate)
    add_mate(0)

    def add_pairs(step):
        total = own[step, pair_at].astype(jnp.float32)
        for hop in range(1, half):
            pair_copy(step, hop).wait_recv()
            total = total + from_pair[step, hop - 1].astype(jnp.float32)
        final[step] = total.astype(jnp.bfloat16)

    def send_row(step):
        add_pairs(step)
        row_copy(step).start()

    loop(1, sp_count, send_row)
    add_pairs(0)
    keep = pltpu.make_async_copy(final.at[0], result_ref.at[sp_at], own_sem)
    keep.start()
    keep.wait()

    def finish(step):
        mate_copy(step).wait_send()
        for hop in range(1, half):
            pair_copy(step, hop).wait_send()

    loop(0, sp_count, finish)

    def finish_rows(step):
        row_arrival(step).wait_recv()
        row_copy(step).wait_send()

    loop(1, sp_count, finish_rows)


def bring_back(partial, collective_id):
    sp_count, half, sides, rows, width = partial.shape
    tp_count = half * sides
    sems = pltpu.SemaphoreType.DMA
    return pl.pallas_call(
        functools.partial(bring_kernel, sp_count, tp_count),
        out_shape=jax.ShapeDtypeStruct((sp_count, rows, width), partial.dtype),
        in_specs=[pl.BlockSpec(memory_space=pl.ANY)],
        out_specs=pl.BlockSpec(memory_space=pl.ANY),
        scratch_shapes=[
            pltpu.VMEM((sp_count, half, rows, width), partial.dtype),
            pltpu.VMEM((sp_count, half, rows, width), partial.dtype),
            pltpu.VMEM((sp_count, max(1, half - 1), rows, width), partial.dtype),
            pltpu.VMEM((sp_count, rows, width), partial.dtype),
            sems((sp_count,)),
            sems((sp_count,)),
            sems((sp_count,)),
            sems((sp_count, half)),
            sems((sp_count, half)),
            sems((sp_count,)),
            sems((sp_count,)),
            sems,
        ],
        compiler_params=pltpu.CompilerParams(collective_id=collective_id, has_side_effects=True),
    )(partial)


def slot_choice(ids, experts, capacity):
    tokens, top_count = ids.shape
    onehots = [ids[:, k : k + 1] == jnp.arange(experts, dtype=jnp.int32)[None, :] for k in range(top_count)]
    named = sum(onehot.astype(jnp.bfloat16) for onehot in onehots)
    order = jnp.arange(tokens, dtype=jnp.int32)
    earlier = (order[None, :] < order[:, None]).astype(jnp.bfloat16)
    ranks = jnp.dot(earlier, named, preferred_element_type=jnp.float32).astype(jnp.int32)
    places = ranks + capacity * jnp.arange(experts, dtype=jnp.int32)[None, :]
    slots = jnp.arange(experts * capacity, dtype=jnp.int32)[None, :]
    return [
        (jnp.sum(jnp.where(onehot, places, 0), axis=1, keepdims=True) == slots).astype(jnp.bfloat16)
        for onehot in onehots
    ]


def expert_work(rows_in, cot_rows, gate_w, up_w, down_w):
    gate_pre = jnp.dot(rows_in, gate_w, preferred_element_type=jnp.float32)
    up_pre = jnp.dot(rows_in, up_w, preferred_element_type=jnp.float32)
    gate_sig = jax.nn.sigmoid(gate_pre)
    gate_act = gate_pre * gate_sig
    hidden = (gate_act * up_pre).astype(jnp.bfloat16)
    down_grad = lax.dot_general(
        hidden, cot_rows, (((0,), (0,)), ((), ())), preferred_element_type=jnp.float32
    )
    grad_hidden = lax.dot_general(
        cot_rows, down_w, (((1,), (1,)), ((), ())), preferred_element_type=jnp.float32
    )
    up_grad = (grad_hidden * gate_act).astype(jnp.bfloat16)
    gate_grad = (grad_hidden * up_pre * gate_sig * (1.0 + gate_pre * (1.0 - gate_sig))).astype(
        jnp.bfloat16
    )
    gate_wgrad = lax.dot_general(
        rows_in, gate_grad, (((0,), (0,)), ((), ())), preferred_element_type=jnp.float32
    )
    up_wgrad = lax.dot_general(
        rows_in, up_grad, (((0,), (0,)), ((), ())), preferred_element_type=jnp.float32
    )
    grads_pair = jnp.stack([gate_grad, up_grad], axis=1)
    weights_pair = jnp.stack([gate_w, up_w], axis=1)
    back_rows = lax.dot_general(
        grads_pair, weights_pair, (((1, 2), (1, 2)), ((), ())), preferred_element_type=jnp.float32
    ).astype(jnp.bfloat16)
    return (gate_wgrad, up_wgrad, down_grad, back_rows)


def pick(choice, rows):
    return lax.dot_general(
        choice, rows, (((0,), (0,)), ((), ())), preferred_element_type=jnp.float32
    ).astype(jnp.bfloat16)


def shards(
    stream_in,
    stream_cot,
    route_ids,
    route_wts,
    norm_gain,
    w_gate,
    w_up,
    w_down,
    out_proj,
    conv_b,
    conv_c,
    conv_h,
    conv_taps,
):
    tp_count = lax.axis_size("tp")
    sp_count = lax.axis_size("sp")
    tp_index = lax.axis_index("tp")
    tok_rows, model_width = stream_in.shape
    top_count = route_ids.shape[1]
    capacity = max(2, 5 * top_count * tok_rows // (4 * sp_count))
    inputs = stream_in.astype(jnp.float32)
    inv_rms = lax.rsqrt(jnp.mean(inputs * inputs, axis=1, keepdims=True) + epsilon)
    scaled = inputs * inv_rms
    normed = (scaled * norm_gain[None, :]).astype(jnp.bfloat16)
    own_ids = lax.dynamic_slice_in_dim(route_ids, tp_index * tok_rows, tok_rows, 0)
    own_wts = lax.dynamic_slice_in_dim(route_wts, tp_index * tok_rows, tok_rows, 0)
    choice = slot_choice(own_ids, sp_count, capacity)
    chosen = sum(choice)
    cot = stream_cot.astype(jnp.float32)
    weighted = jnp.concatenate(
        [(own_wts[:, k : k + 1] * cot).astype(jnp.bfloat16) for k in range(top_count)], axis=0
    )
    buffer_rows = pick(chosen, normed).reshape(sp_count, capacity, model_width)
    buffer_cot = pick(jnp.concatenate(choice, axis=0), weighted).reshape(
        sp_count, capacity, model_width
    )
    edge_rows = 8
    arrived_rows, arrived_cot, c_before, h_before, b_after = spread(
        sp_count,
        tp_count,
        [buffer_rows, buffer_cot],
        [],
        [(conv_c, 1), (conv_h, 1), (conv_b, -1)],
        [],
        edge_rows,
        1,
    )
    gate_wgrad, up_wgrad, down_grad, back_rows = expert_work(
        arrived_rows.reshape(-1, model_width),
        arrived_cot.reshape(-1, model_width),
        w_gate[0],
        w_up[0],
        w_down[0],
    )
    returned = bring_back(
        back_rows.reshape(sp_count, tp_count // 2, 2, capacity, model_width), 2
    )
    grad_normed = jnp.dot(
        chosen,
        returned.reshape(sp_count * capacity, model_width),
        preferred_element_type=jnp.float32,
    )
    q_term = grad_normed * norm_gain[None, :]
    stream_grad = (
        stream_cot.astype(jnp.float32)
        + inv_rms * (q_term - scaled * jnp.mean(q_term * scaled, axis=1, keepdims=True))
    ).astype(jnp.bfloat16)
    feature_blocks = stream_grad.reshape(tok_rows, sp_count, -1).transpose(1, 0, 2)
    rim = conv_taps.shape[0] - 1
    has_before = lax.axis_index("sp") > 0
    gate_ext = jnp.concatenate([c_before[-rim:], conv_c], axis=0).astype(jnp.float32)
    value_ext = jnp.concatenate([h_before[-rim:], conv_h], axis=0).astype(jnp.float32)
    inside = has_before | (jnp.arange(gate_ext.shape[0])[:, None] >= rim)
    conv_in = jnp.where(inside, gate_ext * value_ext, 0.0)
    conv_out = (
        conv_taps[0][None, :] * conv_in[:-2]
        + conv_taps[1][None, :] * conv_in[1:-1]
        + conv_taps[2][None, :] * conv_in[2:]
    )
    mixed = (conv_b.astype(jnp.float32) * conv_out).astype(jnp.bfloat16)
    own_features, group_grad, all_mixed, edge_grad = spread(
        sp_count, tp_count, [feature_blocks], [stream_grad], [], [mixed], edge_rows, 3
    )
    group_grad = group_grad.reshape(-1, model_width)
    grad_mix = lax.dot_general(
        group_grad, out_proj, (((1,), (1,)), ((), ())), preferred_element_type=jnp.float32
    ).astype(jnp.bfloat16)
    all_mixed = all_mixed.reshape(-1, all_mixed.shape[-1])
    proj_grad = lax.dot_general(
        own_features.reshape(all_mixed.shape[0], -1),
        all_mixed,
        (((0,), (0,)), ((), ())),
        preferred_element_type=jnp.float32,
    )
    grad_b = (grad_mix.astype(jnp.float32) * conv_out).astype(jnp.bfloat16)
    edge_mix = lax.dot_general(
        edge_grad, out_proj, (((1,), (1,)), ((), ())), preferred_element_type=jnp.float32
    ).astype(jnp.bfloat16)
    conv_grad = grad_mix.astype(jnp.float32) * conv_b.astype(jnp.float32)
    next_grad = edge_mix.astype(jnp.float32) * b_after.astype(jnp.float32)
    has_after = lax.axis_index("sp") < sp_count - 1
    next_grad = jnp.where(has_after, next_grad, 0.0)[:rim]
    grad_ext = jnp.concatenate([conv_grad, next_grad], axis=0)
    grad_in = (
        conv_taps[2][None, :] * grad_ext[:-2]
        + conv_taps[1][None, :] * grad_ext[1:-1]
        + conv_taps[0][None, :] * grad_ext[2:]
    )
    grad_c = (grad_in * conv_h.astype(jnp.float32)).astype(jnp.bfloat16)
    grad_h = (grad_in * conv_c.astype(jnp.float32)).astype(jnp.bfloat16)
    return (gate_wgrad[None], up_wgrad[None], down_grad[None], proj_grad, grad_b, grad_c, grad_h)


def solution(mesh):
    in_specs = (
        P(("sp", "tp"), None),
        P(("sp", "tp"), None),
        P("sp", None),
        P("sp", None),
        P(),
        P("sp", None, "tp"),
        P("sp", None, "tp"),
        P("sp", "tp", None),
        P("tp", None),
        P("sp", "tp"),
        P("sp", "tp"),
        P("sp", "tp"),
        P(None, "tp"),
    )
    out_specs = (
        P("sp", None, "tp"),
        P("sp", None, "tp"),
        P("sp", "tp", None),
        P("sp", "tp"),
        P("sp", "tp"),
        P("sp", "tp"),
        P("sp", "tp"),
    )
    return jax.shard_map(shards, mesh=mesh, in_specs=in_specs, out_specs=out_specs, check_vma=False)
```

```python
import functools

import jax
import jax.numpy as jnp
from jax import lax
from jax.experimental import pallas as pl
from jax.experimental.pallas import tpu as pltpu
from jax.sharding import PartitionSpec as P

epsilon = 1e-06


def here():
    return lax.axis_index("sp"), lax.axis_index("tp")


def greet(sp_count, tp_count):
    sp_at, tp_at = here()
    half = tp_count // 2
    barrier = pltpu.get_barrier_semaphore()

    def hail(sp_to, tp_to):
        pl.semaphore_signal(
            barrier, inc=1, device_id=(sp_to, tp_to), device_id_type=pl.DeviceIdType.MESH
        )

    def hail_row(step, carry):
        hail(lax.rem(sp_at + step, sp_count), tp_at)
        return carry

    lax.fori_loop(1, sp_count, hail_row, 0)
    for step in range(1, half):
        hail(sp_at, pair_peer(tp_at, step, half))
    hail(sp_at, mate_of(tp_at))
    pl.semaphore_wait(barrier, sp_count - 1 + half)


def pair_peer(tp_at, step, half):
    return lax.rem(tp_at // 2 + step, half) * 2 + lax.rem(tp_at, 2)


def partner(at, step, count):
    other = lax.rem(count - step, count)
    total, bit = 0, 1
    while bit < count:
        total = total + bit * lax.rem(at // bit + other // bit, 2)
        bit *= 2
    return total


def mate_of(tp_at):
    return tp_at + 1 - 2 * lax.rem(tp_at, 2)


def remote(source, target, send_sem, recv_sem, sp_to, tp_to):
    return pltpu.make_async_remote_copy(
        src_ref=source,
        dst_ref=target,
        send_sem=send_sem,
        recv_sem=recv_sem,
        device_id=(sp_to, tp_to),
        device_id_type=pl.DeviceIdType.MESH,
    )


def loop(first, last, body):
    def step(index, carry):
        body(index)
        return carry

    lax.fori_loop(first, last, step, 0)


def spread_kernel(sp_count, tp_count, exchanged, gathered, shifted, lined, edged, *refs):
    count = exchanged + gathered
    moved = len(shifted)
    total = count + moved + lined
    sources, results = refs[:count], refs[total : total + count]
    shift_sources, shift_results = refs[count : count + moved], refs[total + count : total + count + moved]
    line_source = refs[total - 1]
    line_result = refs[2 * total - 1]
    edge_result = refs[2 * total]
    (
        own_sem,
        row_send,
        row_recv,
        pair_send,
        pair_recv,
        mate_send,
        mate_recv,
        last_send,
        last_recv,
        shift_send,
        shift_recv,
        line_send,
        line_recv,
        edge_sem,
    ) = refs[2 * total + edged :]
    sp_at, tp_at = here()
    half = tp_count // 2
    mate = mate_of(tp_at)

    def origin(step):
        return lax.rem(sp_at + sp_count - step, sp_count)

    def slot_of(which, step, tp_from):
        if which < exchanged:
            return results[which].at[origin(step), tp_from]
        return results[which].at[tp_from]

    def own_block(which):
        return sources[which].at[sp_at] if which < exchanged else sources[which]

    def row_copy(which, step):
        to = lax.rem(sp_at + step, sp_count)
        return remote(
            sources[which].at[to],
            results[which].at[sp_at, tp_at],
            row_send.at[which, step],
            row_recv.at[which, step],
            to,
            tp_at,
        )

    def row_arrival(which, step):
        return remote(
            own_block(which),
            slot_of(which, step, tp_at),
            row_send.at[which, step],
            row_recv.at[which, step],
            origin(step),
            tp_at,
        )

    def pair_copy(which, step, hop, source, tp_from):
        return remote(
            source,
            slot_of(which, step, tp_from),
            pair_send.at[which, step, hop],
            pair_recv.at[which, step, hop],
            sp_at,
            pair_peer(tp_at, hop, half),
        )

    def mate_copy(which, step, source, tp_from):
        return remote(
            source,
            slot_of(which, step, tp_from),
            mate_send.at[which, step],
            mate_recv.at[which, step],
            sp_at,
            mate,
        )

    def last_copy(which, step, hop, tp_from):
        return remote(
            slot_of(which, step, tp_from),
            slot_of(which, step, tp_from),
            last_send.at[which, step, hop],
            last_recv.at[which, step, hop],
            sp_at,
            mate,
        )

    def pair_source(hop):
        return pair_peer(tp_at, half - hop, half)

    def pass_on(which, step, source):
        for hop in range(1, half):
            pair_copy(which, step, hop, source, tp_at).start()
        mate_copy(which, step, source, tp_at).start()

    def pass_last(which, step):
        for hop in range(1, half):
            origin_tp = pair_source(hop)
            pair_copy(which, step, hop, own_block(which), origin_tp).wait_recv()
            last_copy(which, step, hop, origin_tp).start()

    def shift_copy(index):
        to = lax.rem(sp_at + sp_count + shifted[index], sp_count)
        rows = shift_results[index].shape[0]
        first = shift_sources[index].shape[0] - rows if shifted[index] > 0 else 0
        return remote(
            shift_sources[index].at[pl.ds(first, rows)],
            shift_results[index],
            shift_send.at[index],
            shift_recv.at[index],
            to,
            tp_at,
        )

    edge_rows = edge_result.shape[0] if edged else 0

    def edge_copy():
        return remote(
            results[exchanged].at[0, pl.ds(0, edge_rows)],
            edge_result,
            edge_sem.at[0],
            edge_sem.at[1],
            lax.rem(sp_at + sp_count - 1, sp_count),
            tp_at,
        )

    depth = sp_count // 2
    deep, lane = sp_at // 2, lax.rem(sp_at, 2)

    def line_slot(where, side):
        return line_result.at[where * 2 + side]

    def line_copy(way, step):
        toward = 1 - 2 * way
        where = jnp.clip(deep - toward * step, 0, depth - 1)
        return remote(
            line_slot(where, lane),
            line_slot(where, lane),
            line_send.at[way, step],
            line_recv.at[way, step + 1],
            jnp.clip(deep + toward, 0, depth - 1) * 2 + lane,
            tp_at,
        )

    def line_arrival(way, step):
        toward = 1 - 2 * way
        where = jnp.clip(deep - toward * step, 0, depth - 1)
        return remote(
            line_slot(where, lane),
            line_slot(where, lane),
            line_send.at[way, step],
            line_recv.at[way, step],
            jnp.clip(deep - toward, 0, depth - 1) * 2 + lane,
            tp_at,
        )

    def line_mate(where, side):
        return remote(
            line_slot(where, side),
            line_slot(where, side),
            line_send.at[2, where],
            line_recv.at[2, where],
            deep * 2 + 1 - lane,
            tp_at,
        )

    def reach(way):
        return deep if way == 0 else depth - 1 - deep

    def line_pass(way, step):
        @pl.when(reach(1 - way) > 0)
        def _():
            line_copy(way, step).start()

    def line_step(step):
        for way in range(2):

            @pl.when(step <= reach(way))
            def _():
                line_arrival(way, step).wait_recv()
                line_pass(way, step)
                toward = 1 - 2 * way
                line_mate(jnp.clip(deep - toward * step, 0, depth - 1), lane).start()

    greet(sp_count, tp_count)
    for index in range(moved):
        shift_copy(index).start()
    if lined:
        line_own = pltpu.make_async_copy(line_source, line_slot(deep, lane), edge_sem.at[2])
        line_own.start()
    for which in range(exchanged):
        loop(1, sp_count, lambda step: row_copy(which, step).start())
    locals_ = [
        pltpu.make_async_copy(own_block(which), slot_of(which, 0, tp_at), own_sem.at[which])
        for which in range(count)
    ]
    for copy in locals_:
        copy.start()
    for which in reversed(range(count)):
        pass_on(which, 0, own_block(which))

    if lined:
        line_own.wait()
        for way in range(2):
            line_pass(way, 0)
        line_mate(deep, lane).start()
    for which in range(exchanged, count):
        pass_last(which, 0)
    for which in range(exchanged):

        def relay(step, before):
            row_arrival(which, step).wait_recv()
            pass_on(which, step, slot_of(which, step, tp_at))
            pass_last(which, before)

        def relay_at(place):
            relay(place, place - 1)
            if lined and which == 0:

                @pl.when(lax.rem(place, 2) == 0)
                def _():
                    line_step(place // 2)

        loop(1, sp_count, relay_at)
        pass_last(which, sp_count - 1)

    for copy in locals_:
        copy.wait()
    for which in reversed(range(count)):
        steps = sp_count if which < exchanged else 1

        def finish(step):
            for hop in range(1, half):
                pair_copy(which, step, hop, own_block(which), tp_at).wait_send()
                last_copy(which, step, hop, pair_source(hop)).wait_send()
                last_copy(
                    which, step, hop, mate_of(pair_source(hop))
                ).wait_recv()
            mate_copy(which, step, own_block(which), tp_at).wait_send()
            mate_copy(which, step, own_block(which), mate).wait_recv()

        loop(0, steps, finish)
        if which < exchanged:
            loop(1, sp_count, lambda step: row_copy(which, step).wait_send())
        elif edged and which == exchanged:
            edge_copy().start()

    for index in range(moved):
        shift_copy(index).wait()
    if lined:
        for way in range(2):

            @pl.when(reach(1 - way) > 0)
            def _():
                loop(0, reach(way) + 1, lambda step: line_copy(way, step).wait_send())

        def finish_line(where):
            line_mate(where, lane).wait_send()
            line_mate(where, 1 - lane).wait_recv()

        loop(0, depth, finish_line)
    if edged:
        edge_copy().wait()


def spread(sp_count, tp_count, exchanged, gathered, shifted, lined, edge_rows, collective_id):
    arrays = exchanged + gathered + [value for value, _ in shifted] + lined
    count = len(exchanged) + len(gathered)
    half = tp_count // 2
    edged = 1 if edge_rows and gathered else 0
    shapes = (
        [(sp_count, tp_count) + value.shape[1:] for value in exchanged]
        + [(tp_count,) + value.shape for value in gathered]
        + [(edge_rows,) + value.shape[1:] for value, _ in shifted]
        + [(sp_count,) + value.shape for value in lined]
    )
    out_shape = [
        jax.ShapeDtypeStruct(shape, value.dtype) for shape, value in zip(shapes, arrays)
    ]
    if edged:
        out_shape.append(
            jax.ShapeDtypeStruct((edge_rows, gathered[0].shape[1]), gathered[0].dtype)
        )
    sems = pltpu.SemaphoreType.DMA
    return pl.pallas_call(
        functools.partial(
            spread_kernel,
            sp_count,
            tp_count,
            len(exchanged),
            len(gathered),
            tuple(step for _, step in shifted),
            len(lined),
            edged,
        ),
        out_shape=tuple(out_shape),
        in_specs=[pl.BlockSpec(memory_space=pltpu.VMEM)] * count
        + [pl.BlockSpec(memory_space=pl.ANY)] * len(shifted)
        + [pl.BlockSpec(memory_space=pltpu.VMEM)] * len(lined),
        out_specs=tuple([pl.BlockSpec(memory_space=pl.ANY)] * len(out_shape)),
        scratch_shapes=[sems((count,))]
        + [sems((count, sp_count))] * 2
        + [sems((count, sp_count, half))] * 2
        + [sems((count, sp_count))] * 2
        + [sems((count, sp_count, half))] * 2
        + [sems((max(1, len(shifted)),))] * 2
        + [sems((3, sp_count // 2 + 1))] * 2
        + [sems((3,))],
        compiler_params=pltpu.CompilerParams(collective_id=collective_id, has_side_effects=True),
    )(*arrays)


def bring_kernel(
    sp_count,
    tp_count,
    partial_ref,
    result_ref,
    own,
    from_mate,
    from_pair,
    final,
    load_sem,
    mate_send,
    mate_recv,
    pair_send,
    pair_recv,
    row_send,
    row_recv,
    own_sem,
):
    sp_at, tp_at = here()
    half = tp_count // 2
    pair_at, side = tp_at // 2, lax.rem(tp_at, 2)
    mate = mate_of(tp_at)

    def target(step):
        return partner(sp_at, step, sp_count)

    def load(step):
        return pltpu.make_async_copy(
            partial_ref.at[target(step), :, side], own.at[step], load_sem.at[step]
        )

    def mate_copy(step):
        return remote(
            partial_ref.at[target(step), :, 1 - side],
            from_mate.at[step],
            mate_send.at[step],
            mate_recv.at[step],
            sp_at,
            mate,
        )

    def pair_copy(step, hop):
        return remote(
            own.at[step, lax.rem(pair_at + hop, half)],
            from_pair.at[step, hop - 1],
            pair_send.at[step, hop],
            pair_recv.at[step, hop],
            sp_at,
            pair_peer(tp_at, hop, half),
        )

    def row_copy(step):
        return remote(
            final.at[step],
            result_ref.at[sp_at],
            row_send.at[step],
            row_recv.at[step],
            target(step),
            tp_at,
        )

    def row_arrival(step):
        came = target(step)
        return remote(
            final.at[step],
            result_ref.at[came],
            row_send.at[step],
            row_recv.at[step],
            came,
            tp_at,
        )

    greet(sp_count, tp_count)

    def begin(step):
        mate_copy(step).start()
        load(step).start()

    loop(1, sp_count, begin)
    begin(0)

    def add_mate(step):
        load(step).wait()
        mate_copy(step).wait_recv()
        own[step] = (
            own[step].astype(jnp.float32) + from_mate[step].astype(jnp.float32)
        ).astype(jnp.bfloat16)
        for hop in range(1, half):
            pair_copy(step, hop).start()

    loop(1, sp_count, add_mate)
    add_mate(0)

    def add_pairs(step):
        total = own[step, pair_at].astype(jnp.float32)
        for hop in range(1, half):
            pair_copy(step, hop).wait_recv()
            total = total + from_pair[step, hop - 1].astype(jnp.float32)
        final[step] = total.astype(jnp.bfloat16)

    def send_row(step):
        add_pairs(step)
        row_copy(step).start()

    loop(1, sp_count, send_row)
    add_pairs(0)
    keep = pltpu.make_async_copy(final.at[0], result_ref.at[sp_at], own_sem)
    keep.start()
    keep.wait()

    def finish(step):
        mate_copy(step).wait_send()
        for hop in range(1, half):
            pair_copy(step, hop).wait_send()

    loop(0, sp_count, finish)

    def finish_rows(step):
        row_arrival(step).wait_recv()
        row_copy(step).wait_send()

    loop(1, sp_count, finish_rows)


def bring_back(partial, collective_id):
    sp_count, half, sides, rows, width = partial.shape
    tp_count = half * sides
    sems = pltpu.SemaphoreType.DMA
    return pl.pallas_call(
        functools.partial(bring_kernel, sp_count, tp_count),
        out_shape=jax.ShapeDtypeStruct((sp_count, rows, width), partial.dtype),
        in_specs=[pl.BlockSpec(memory_space=pl.ANY)],
        out_specs=pl.BlockSpec(memory_space=pl.ANY),
        scratch_shapes=[
            pltpu.VMEM((sp_count, half, rows, width), partial.dtype),
            pltpu.VMEM((sp_count, half, rows, width), partial.dtype),
            pltpu.VMEM((sp_count, max(1, half - 1), rows, width), partial.dtype),
            pltpu.VMEM((sp_count, rows, width), partial.dtype),
            sems((sp_count,)),
            sems((sp_count,)),
            sems((sp_count,)),
            sems((sp_count, half)),
            sems((sp_count, half)),
            sems((sp_count,)),
            sems((sp_count,)),
            sems,
        ],
        compiler_params=pltpu.CompilerParams(collective_id=collective_id, has_side_effects=True),
    )(partial)


def slot_choice(ids, experts, capacity):
    tokens, top_count = ids.shape
    onehots = [ids[:, k : k + 1] == jnp.arange(experts, dtype=jnp.int32)[None, :] for k in range(top_count)]
    named = sum(onehot.astype(jnp.bfloat16) for onehot in onehots)
    order = jnp.arange(tokens, dtype=jnp.int32)
    earlier = (order[None, :] < order[:, None]).astype(jnp.bfloat16)
    ranks = jnp.dot(earlier, named, preferred_element_type=jnp.float32).astype(jnp.int32)
    places = ranks + capacity * jnp.arange(experts, dtype=jnp.int32)[None, :]
    slots = jnp.arange(experts * capacity, dtype=jnp.int32)[None, :]
    return [
        (jnp.sum(jnp.where(onehot, places, 0), axis=1, keepdims=True) == slots).astype(jnp.bfloat16)
        for onehot in onehots
    ]


def expert_work(rows_in, cot_rows, gate_w, up_w, down_w):
    gate_pre = jnp.dot(rows_in, gate_w, preferred_element_type=jnp.float32)
    up_pre = jnp.dot(rows_in, up_w, preferred_element_type=jnp.float32)
    gate_sig = jax.nn.sigmoid(gate_pre)
    gate_act = gate_pre * gate_sig
    hidden = (gate_act * up_pre).astype(jnp.bfloat16)
    down_grad = lax.dot_general(
        hidden, cot_rows, (((0,), (0,)), ((), ())), preferred_element_type=jnp.float32
    )
    grad_hidden = lax.dot_general(
        cot_rows, down_w, (((1,), (1,)), ((), ())), preferred_element_type=jnp.float32
    )
    up_grad = (grad_hidden * gate_act).astype(jnp.bfloat16)
    gate_grad = (grad_hidden * up_pre * gate_sig * (1.0 + gate_pre * (1.0 - gate_sig))).astype(
        jnp.bfloat16
    )
    gate_wgrad = lax.dot_general(
        rows_in, gate_grad, (((0,), (0,)), ((), ())), preferred_element_type=jnp.float32
    )
    up_wgrad = lax.dot_general(
        rows_in, up_grad, (((0,), (0,)), ((), ())), preferred_element_type=jnp.float32
    )
    grads_pair = jnp.stack([gate_grad, up_grad], axis=1)
    weights_pair = jnp.stack([gate_w, up_w], axis=1)
    back_rows = lax.dot_general(
        grads_pair, weights_pair, (((1, 2), (1, 2)), ((), ())), preferred_element_type=jnp.float32
    ).astype(jnp.bfloat16)
    return (gate_wgrad, up_wgrad, down_grad, back_rows)


def pick(choice, rows):
    return lax.dot_general(
        choice, rows, (((0,), (0,)), ((), ())), preferred_element_type=jnp.float32
    ).astype(jnp.bfloat16)


def shards(
    stream_in,
    stream_cot,
    route_ids,
    route_wts,
    norm_gain,
    w_gate,
    w_up,
    w_down,
    out_proj,
    conv_b,
    conv_c,
    conv_h,
    conv_taps,
):
    tp_count = lax.axis_size("tp")
    sp_count = lax.axis_size("sp")
    tp_index = lax.axis_index("tp")
    tok_rows, model_width = stream_in.shape
    top_count = route_ids.shape[1]
    capacity = max(2, 5 * top_count * tok_rows // (4 * sp_count))
    inputs = stream_in.astype(jnp.float32)
    inv_rms = lax.rsqrt(jnp.mean(inputs * inputs, axis=1, keepdims=True) + epsilon)
    scaled = inputs * inv_rms
    normed = (scaled * norm_gain[None, :]).astype(jnp.bfloat16)
    own_ids = lax.dynamic_slice_in_dim(route_ids, tp_index * tok_rows, tok_rows, 0)
    own_wts = lax.dynamic_slice_in_dim(route_wts, tp_index * tok_rows, tok_rows, 0)
    choice = slot_choice(own_ids, sp_count, capacity)
    chosen = sum(choice)
    cot = stream_cot.astype(jnp.float32)
    weighted = jnp.concatenate(
        [(own_wts[:, k : k + 1] * cot).astype(jnp.bfloat16) for k in range(top_count)], axis=0
    )
    buffer_rows = pick(chosen, normed).reshape(sp_count, capacity, model_width)
    buffer_cot = pick(jnp.concatenate(choice, axis=0), weighted).reshape(
        sp_count, capacity, model_width
    )
    edge_rows = 8
    arrived_rows, arrived_cot, c_before, h_before, b_after = spread(
        sp_count,
        tp_count,
        [buffer_rows, buffer_cot],
        [],
        [(conv_c, 1), (conv_h, 1), (conv_b, -1)],
        [],
        edge_rows,
        1,
    )
    gate_wgrad, up_wgrad, down_grad, back_rows = expert_work(
        arrived_rows.reshape(-1, model_width),
        arrived_cot.reshape(-1, model_width),
        w_gate[0],
        w_up[0],
        w_down[0],
    )
    returned = bring_back(
        back_rows.reshape(sp_count, tp_count // 2, 2, capacity, model_width), 2
    )
    grad_normed = jnp.dot(
        chosen,
        returned.reshape(sp_count * capacity, model_width),
        preferred_element_type=jnp.float32,
    )
    q_term = grad_normed * norm_gain[None, :]
    stream_grad = (
        stream_cot.astype(jnp.float32)
        + inv_rms * (q_term - scaled * jnp.mean(q_term * scaled, axis=1, keepdims=True))
    ).astype(jnp.bfloat16)
    feature_blocks = stream_grad.reshape(tok_rows, sp_count, -1).transpose(1, 0, 2)
    rim = conv_taps.shape[0] - 1
    has_before = lax.axis_index("sp") > 0
    gate_ext = jnp.concatenate([c_before[-rim:], conv_c], axis=0).astype(jnp.float32)
    value_ext = jnp.concatenate([h_before[-rim:], conv_h], axis=0).astype(jnp.float32)
    inside = has_before | (jnp.arange(gate_ext.shape[0])[:, None] >= rim)
    conv_in = jnp.where(inside, gate_ext * value_ext, 0.0)
    conv_out = (
        conv_taps[0][None, :] * conv_in[:-2]
        + conv_taps[1][None, :] * conv_in[1:-1]
        + conv_taps[2][None, :] * conv_in[2:]
    )
    mixed = (conv_b.astype(jnp.float32) * conv_out).astype(jnp.bfloat16)
    own_features, group_grad, all_mixed, edge_grad = spread(
        sp_count, tp_count, [feature_blocks], [stream_grad], [], [mixed], edge_rows, 3
    )
    group_grad = group_grad.reshape(-1, model_width)
    grad_mix = lax.dot_general(
        group_grad, out_proj, (((1,), (1,)), ((), ())), preferred_element_type=jnp.float32
    ).astype(jnp.bfloat16)
    all_mixed = all_mixed.reshape(-1, all_mixed.shape[-1])
    proj_grad = lax.dot_general(
        own_features.reshape(all_mixed.shape[0], -1),
        all_mixed,
        (((0,), (0,)), ((), ())),
        preferred_element_type=jnp.float32,
    )
    grad_b = (grad_mix.astype(jnp.float32) * conv_out).astype(jnp.bfloat16)
    edge_mix = lax.dot_general(
        edge_grad, out_proj, (((1,), (1,)), ((), ())), preferred_element_type=jnp.float32
    ).astype(jnp.bfloat16)
    conv_grad = grad_mix.astype(jnp.float32) * conv_b.astype(jnp.float32)
    next_grad = edge_mix.astype(jnp.float32) * b_after.astype(jnp.float32)
    has_after = lax.axis_index("sp") < sp_count - 1
    next_grad = jnp.where(has_after, next_grad, 0.0)[:rim]
    grad_ext = jnp.concatenate([conv_grad, next_grad], axis=0)
    grad_in = (
        conv_taps[2][None, :] * grad_ext[:-2]
        + conv_taps[1][None, :] * grad_ext[1:-1]
        + conv_taps[0][None, :] * grad_ext[2:]
    )
    grad_c = (grad_in * conv_h.astype(jnp.float32)).astype(jnp.bfloat16)
    grad_h = (grad_in * conv_c.astype(jnp.float32)).astype(jnp.bfloat16)
    return (gate_wgrad[None], up_wgrad[None], down_grad[None], proj_grad, grad_b, grad_c, grad_h)


def solution(mesh):
    in_specs = (
        P(("sp", "tp"), None),
        P(("sp", "tp"), None),
        P("sp", None),
        P("sp", None),
        P(),
        P("sp", None, "tp"),
        P("sp", None, "tp"),
        P("sp", "tp", None),
        P("tp", None),
        P("sp", "tp"),
        P("sp", "tp"),
        P("sp", "tp"),
        P(None, "tp"),
    )
    out_specs = (
        P("sp", None, "tp"),
        P("sp", None, "tp"),
        P("sp", "tp", None),
        P("sp", "tp"),
        P("sp", "tp"),
        P("sp", "tp"),
        P("sp", "tp"),
    )
    return jax.shard_map(shards, mesh=mesh, in_specs=in_specs, out_specs=out_specs, check_vma=False)
```
